256 devices in a mesh: grp: 2 (over y), sp: 32 (over z, core), tp: 4 (over x).
Axes of the slice: x: 4, y: 2, z: 16, core: 2. Of those that a mesh axis runs over, the one named last changes fastest.
The devices are a block of a 4x16x16 slice.
Arguments:
- queries_a: bfloat16 [16384, 2, 512], P(('grp', 'sp'), None, 'tp'), parts along dimension 0, may hold values from -120 to 120
- keys_a: bfloat16 [16384, 2, 512], P(('grp', 'sp'), None, 'tp'), parts along dimension 0, may hold values from -6 to 6
- values_a: bfloat16 [16384, 1024], P(('grp', 'sp'), 'tp'), parts along dimension 0, may hold values from -6 to 6
- queries_b: bfloat16 [16384, 2, 512], P(('grp', 'sp'), None, 'tp'), parts along dimension 0, may hold values from -120 to 120
- keys_b: bfloat16 [16384, 2, 512], P(('grp', 'sp'), None, 'tp'), parts along dimension 0, may hold values from -6 to 6
- values_b: bfloat16 [16384, 1024], P(('grp', 'sp'), 'tp'), parts along dimension 0, may hold values from -6 to 6
- lambdas: float32 [12], replicated, may hold values from 0.3 to 0.8
- head_gain_a: float32 [256], replicated, may hold values from 0.1 to 1.9
- head_gain_b: float32 [128], replicated, may hold values from 0.1 to 1.9
- out_a: bfloat16 [1024, 2048], P('tp'), may hold values from -0.125 to 0.125
- out_b: bfloat16 [1024, 2048], P('tp'), may hold values from -0.125 to 0.125
- residual: bfloat16 [16384, 2048], P(('grp', 'sp', 'tp')), parts along dimension 0, may hold values from -6 to 6
- gain_mix: float32 [2048], replicated, may hold values from 0.1 to 1.9
- gain_pre: float32 [2048], replicated, may hold values from 0.1 to 1.9
- gain_post: float32 [2048], replicated, may hold values from 0.1 to 1.9
- routes: int32 [16384, 4], P(('grp', 'sp', 'tp')), parts along dimension 0, may hold values from 0 to 31, all different within a row; in each aligned block of 64 rows (0 to 63, 64 to 127, ...) at most 10 rows name the same one
- route_weights: float32 [16384, 4], P(('grp', 'sp', 'tp')), parts along dimension 0, may hold values from 0.05 to 1
- expert_gate: bfloat16 [32, 2048, 2048], P('sp', None, 'tp'), may hold values from -1 to 1
- expert_up: bfloat16 [32, 2048, 2048], P('sp', None, 'tp'), may hold values from -1 to 1
- expert_down: bfloat16 [32, 2048, 2048], P('sp', 'tp'), may hold values from -0.125 to 0.125
Outputs:
- layer_out: bfloat16 [16384, 2048], P(('grp', 'sp', 'tp')), parts along dimension 0
The draws below stay inside these ranges and needn't reach their ends.
There are 2 independent parts, one for each index of `grp`. The reference program is written for one: setup_inputs(seed, part) draws one part's arguments, and reference() takes and returns one part's arrays. A program takes and returns all parts, laid end to end along the dimension named above; an argument that names none is the same for every part. Nothing has to cross between parts.
Inputs may be any that keep to these rules, and one draw needn't show every extreme that they name: `routes`: in each aligned block of 64 rows (the rows of one device) no expert is named by more than 10 rows, a bound that some blocks reach.
All inputs are finite; a program needn't handle non-finite values.
Results may differ from the reference program's by a relative error of at most 0.018.
Values may be sent and summed in bfloat16 or wider, within the bound.
No kernel may reach another device: no remote copies, remote signals or barrier semaphores. Data moves between devices by JAX's collectives and lax.ppermute only.
A program may use at most 128 MiB of HBM per device.

```python
import math
import jax
import jax.numpy as jnp
import numpy as np
from jax import lax

HA = 4
HB = 8
DA = 128
DB = 64
D = 2048
FF = 2048
TOP_K = 4
TOK_DEV = 256
TOKENS = 8192
TOKSUB = 64
EXPERTS = 32
CAP = 10
N_TP = 4


def pair_fields(key, salt, width):
    keys = jnp.clip(jax.random.normal(jax.random.fold_in(key, salt), (TOKENS, 2, width), jnp.float32) * 1.32, -6.0, 6.0)
    queries = jnp.clip(jax.random.normal(jax.random.fold_in(key, salt + 1), (TOKENS, 2, width), jnp.float32) * 1.32, -6.0, 6.0)
    return (queries, keys)


def draw_queries_a(key, part):
    queries, keys = pair_fields(key, 11, HA * DA)
    return queries.astype(jnp.bfloat16)


def draw_keys_a(key, part):
    queries, keys = pair_fields(key, 11, HA * DA)
    return keys.astype(jnp.bfloat16)


def draw_queries_b(key, part):
    queries, keys = pair_fields(key, 21, HB * DB)
    return queries.astype(jnp.bfloat16)


def draw_keys_b(key, part):
    queries, keys = pair_fields(key, 21, HB * DB)
    return keys.astype(jnp.bfloat16)


def expert_field(key, salt):
    base = jnp.clip(jax.random.normal(jax.random.fold_in(key, salt), (EXPERTS, D, FF), jnp.float32), -6.0, 6.0)
    factor = 1.0
    return jnp.clip(base * factor / jnp.sqrt(jnp.float32(D)), -1.0, 1.0)


def draw_expert_gate(key, part):
    return expert_field(key, 31).astype(jnp.bfloat16)


def draw_expert_up(key, part):
    return expert_field(key, 37).astype(jnp.bfloat16)


def block_scale(key, dims, cuts, smallest, high):
    def one(position, parts):
        heights = jax.random.uniform(jax.random.fold_in(jax.random.fold_in(key, 6), position), (parts,), jnp.float32, smallest / len(cuts), high / len(cuts))
        return jnp.repeat(jnp.exp(heights), dims[position] // parts).reshape((-1,) + (1,) * (len(dims) - position - 1))

    loudness = one(*cuts[0])
    for cut in cuts[1:]:
        loudness = loudness * one(*cut)
    return loudness


def assign_block(key, own, number, rows, amount, top, most, skew):
    ranking = jax.random.permutation(key, amount)
    packed, common = load_shares(amount, rows * top, most, skew, True), load_shares(amount, rows * top, most, skew, False)
    places = jnp.arange(amount)

    def named(lengths, rotation):
        used = int((lengths > 0).sum())
        fixed = max(1, used // 4)
        moved = fixed + (places - fixed + rotation * (used - fixed)) % max(1, amount - fixed)
        return jnp.zeros((amount,), jnp.int32).at[ranking[jnp.where(places < fixed, places, moved)]].set(jnp.asarray(lengths, jnp.int32))

    lengths = jnp.where(number % 4 == 0, named(packed, number // 4), named(common, number - number // 4 - 1))
    mixed = jax.random.permutation(jax.random.fold_in(own, 3), amount)
    source_of, sink = mixed[0:amount // 2 * 2:2], mixed[1:amount // 2 * 2:2]
    room = jnp.minimum(lengths[source_of] - 1, most - lengths[sink]) // 2
    room = jnp.where((source_of == ranking[0]) | (sink == ranking[0]) | (lengths[sink] == 0), 0, jnp.maximum(room, 0))
    moved = jax.random.randint(jax.random.fold_in(own, 4), (amount // 2,), 0, 1 << 20) % (room + 1)
    lengths = lengths.at[source_of].add(-moved).at[sink].add(moved)
    items = jnp.searchsorted(jnp.cumsum(lengths), jnp.arange(rows * top), side="right").astype(jnp.int32)
    grid = items.reshape(top, rows).T
    grid = grid[jax.random.permutation(jax.random.fold_in(own, 1), rows)]
    rotation = jax.random.randint(jax.random.fold_in(own, 2), (rows, 1), 0, top)
    return jnp.take_along_axis(grid, (jnp.arange(top)[None, :] + rotation) % top, axis=1)


def load_shares(amount, total, limit, lean, full):
    weights = [(1 << 20) // math.isqrt(standing ** lean) + 1 for standing in range(1, amount + 1)]
    largest = limit if full else min(limit, max(-(-total // amount), total * weights[0] // sum(weights)))
    least = 1 if total - largest >= amount - 1 else 0
    given, spare = [largest] + [least] * (amount - 1), total - largest - least * (amount - 1)
    while spare > 0:
        candidates = [i for i in range(1, amount) if given[i] < largest] or [i for i in range(1, amount) if given[i] < limit]
        pool, budget = sum([weights[i] for i in candidates]), spare
        for i in candidates:
            extra = min(limit - given[i], max(1, budget * weights[i] // pool), spare)
            given[i] = given[i] + extra
            spare = spare - extra
    return np.array(given)


def centred(stream_key, dims, deviation, most, split=(), kind=jnp.bfloat16):
    drawn = jax.random.normal(stream_key, dims, jnp.float32) * deviation
    if len(split) > 0:
        drawn = block_scale(stream_key, dims, split, -0.22, 0.18) * drawn
    return jnp.clip(drawn, min=-most, max=most).astype(kind)


def setup_inputs(seed: int = 0, part: int = 0) -> dict:
    seeds = jax.random.split(jax.random.key(seed), 21)
    part_splits = jax.random.split(jax.random.fold_in(seeds[20], part), 21)
    queries_a = draw_queries_a(jax.random.fold_in(jax.random.fold_in(seeds[20], part), 71), part)
    keys_a = draw_keys_a(jax.random.fold_in(jax.random.fold_in(seeds[20], part), 71), part)
    values_a = centred(part_splits[2], (TOKENS, HA * 2 * DA), 1.0, 6.0, ((0, 32), (1, 4)))
    queries_b = draw_queries_b(jax.random.fold_in(jax.random.fold_in(seeds[20], part), 71), part)
    keys_b = draw_keys_b(jax.random.fold_in(jax.random.fold_in(seeds[20], part), 71), part)
    values_b = centred(part_splits[5], (TOKENS, HB * 2 * DB), 1.0, 6.0, ((0, 32), (1, 4)))
    lambdas = jnp.clip(jax.random.uniform(seeds[6], (HA + HB,), jnp.float32, 0.3, 0.8), 0.3, 0.8)
    head_gain_a = jnp.clip(1.0 + 0.18 * jax.random.normal(seeds[7], (2 * DA,), jnp.float32), 0.1, 1.9)
    head_gain_b = jnp.clip(1.0 + 0.18 * jax.random.normal(seeds[8], (2 * DB,), jnp.float32), 0.1, 1.9)
    out_a = centred(seeds[9], (HA * 2 * DA, D), D ** -0.5, 0.125, ((0, 4),))
    out_b = centred(seeds[10], (HB * 2 * DB, D), D ** -0.5, 0.125, ((0, 4),))
    residual = centred(part_splits[11], (TOKENS, D), 1.0, 6.0, ((0, 128),))
    gain_mix = jnp.clip(1.0 + 0.18 * jax.random.normal(seeds[12], (D,), jnp.float32), 0.1, 1.9)
    gain_pre = jnp.clip(1.0 + 0.18 * jax.random.normal(seeds[13], (D,), jnp.float32), 0.1, 1.9)
    gain_post = jnp.clip(1.0 + 0.18 * jax.random.normal(seeds[14], (D,), jnp.float32), 0.1, 1.9)
    routes_keys = jax.random.split(jax.random.fold_in(part_splits[15], 1), TOKENS // TOKSUB)
    routes_turns = jax.random.permutation(jax.random.fold_in(part_splits[15], 3), TOKENS // TOKSUB)
    routes = jax.vmap(lambda own, number: assign_block(jax.random.fold_in(part_splits[15], 2), own, number, TOKSUB, EXPERTS, TOP_K, CAP, 1))(routes_keys, routes_turns).reshape((TOKENS, TOP_K))
    route_weights = jnp.clip(0.05 + 0.95 * jax.random.uniform(part_splits[16], (TOKENS, TOP_K), jnp.float32) ** block_scale(part_splits[16], (TOKENS, TOP_K), ((0, 128),), -0.2, 0.2), 0.05, 1.0)
    expert_gate = draw_expert_gate(jax.random.fold_in(seeds[20], 71), part)
    expert_up = draw_expert_up(jax.random.fold_in(seeds[20], 71), part)
    expert_down = centred(seeds[19], (EXPERTS, FF, D), FF ** -0.5, 0.125, ((0, 32), (1, 4)))
    return dict(queries_a=queries_a, keys_a=keys_a, values_a=values_a, queries_b=queries_b, keys_b=keys_b, values_b=values_b, lambdas=lambdas, head_gain_a=head_gain_a, head_gain_b=head_gain_b, out_a=out_a, out_b=out_b, residual=residual, gain_mix=gain_mix, gain_pre=gain_pre, gain_post=gain_post, routes=routes, route_weights=route_weights, expert_gate=expert_gate, expert_up=expert_up, expert_down=expert_down)


def rms_norm(values, gain_vec):
    return values * lax.rsqrt(lax.optimization_barrier(jnp.mean(values * values, -1, keepdims=True)) + 1e-06) * gain_vec.astype(jnp.float32)

def attend_group(queries, keys, values, weights_two, gain_vec, head_size):
    heads = queries.shape[2] // head_size
    query_all = queries.astype(jnp.float32).reshape(TOKENS, 2, heads, head_size)
    key_all = keys.astype(jnp.float32).reshape(TOKENS, 2, heads, head_size)
    value_all = values.astype(jnp.float32).reshape(TOKENS, heads, 2 * head_size)
    span_rows = 512 if TOKENS % 512 == 0 else TOKENS
    key_pos = jnp.arange(TOKENS, dtype=jnp.int32)

    def one_block(first_row):
        query_rows = lax.dynamic_slice_in_dim(query_all, first_row, span_rows, 0)
        query_pos = first_row + jnp.arange(span_rows, dtype=jnp.int32)
        visible = (key_pos[None, :] <= query_pos[:, None])[None, :, None, :]
        scores = jnp.einsum('qmhd,kmhd->mqhk', query_rows, key_all, precision=lax.Precision.HIGHEST) * head_size ** (-0.5)
        scores = jnp.where(visible, scores, -1e+30)
        row_top = lax.optimization_barrier(jnp.max(scores, -1, keepdims=True))
        exp_terms = jnp.where(visible, jnp.exp(scores - row_top), 0.0)
        totals = lax.optimization_barrier(jnp.sum(exp_terms, -1))
        rounded = lax.optimization_barrier(exp_terms.astype(jnp.bfloat16)).astype(jnp.float32)
        accum = jnp.einsum('mqhk,khe->mqhe', rounded, value_all, precision=lax.Precision.HIGHEST)
        mixture = accum[0] / totals[0][..., None] - weights_two[None, :, None] * accum[1] / totals[1][..., None]
        normed = rms_norm(mixture, gain_vec)
        return normed.reshape(span_rows, heads * 2 * head_size).astype(jnp.bfloat16)
    firsts = jnp.arange(0, TOKENS, span_rows, dtype=jnp.int32)
    return lax.map(one_block, firsts).reshape(TOKENS, heads * 2 * head_size)

def slot_numbers(flat_ids):
    onehot = (flat_ids[:, None] == jnp.arange(EXPERTS, dtype=jnp.int32)[None, :]).astype(jnp.int32)
    before = jnp.cumsum(onehot, 0) - onehot
    return lax.optimization_barrier(jnp.sum(before * onehot, 1)).astype(jnp.int32)

def reference(queries_a, keys_a, values_a, queries_b, keys_b, values_b, lambdas, head_gain_a, head_gain_b, out_a, out_b, residual, gain_mix, gain_pre, gain_post, routes, route_weights, expert_gate, expert_up, expert_down):
    heads_out_a = attend_group(queries_a, keys_a, values_a, lambdas[:HA], head_gain_a, DA)
    heads_out_b = attend_group(queries_b, keys_b, values_b, lambdas[HA:], head_gain_b, DB)
    width_a = heads_out_a.shape[1] // N_TP
    width_b = heads_out_b.shape[1] // N_TP
    mixed_rows = jnp.zeros((TOKENS, D), jnp.float32)
    for part_index in range(N_TP):
        part_a = jnp.dot(heads_out_a[:, part_index * width_a:(part_index + 1) * width_a], out_a[part_index * width_a:(part_index + 1) * width_a], preferred_element_type=jnp.float32)
        part_b = jnp.dot(heads_out_b[:, part_index * width_b:(part_index + 1) * width_b], out_b[part_index * width_b:(part_index + 1) * width_b], preferred_element_type=jnp.float32)
        mixed_rows = mixed_rows + lax.optimization_barrier((part_a + part_b).astype(jnp.bfloat16)).astype(jnp.float32)
    after_mix = (residual.astype(jnp.float32) + rms_norm(mixed_rows, gain_mix)).astype(jnp.bfloat16)
    normed = rms_norm(after_mix.astype(jnp.float32), gain_pre).astype(jnp.bfloat16)
    sub_rows = TOK_DEV // N_TP
    blocks = TOKENS // sub_rows
    route_blocks = routes.astype(jnp.int32).reshape(blocks, sub_rows * TOP_K)
    slot_ids = jax.vmap(slot_numbers)(route_blocks)
    block_ids = jnp.broadcast_to(jnp.arange(blocks, dtype=jnp.int32)[:, None], route_blocks.shape)
    token_ids = jnp.repeat(jnp.arange(TOKENS, dtype=jnp.int32).reshape(blocks, sub_rows), TOP_K, axis=1)
    table = jnp.full((EXPERTS, blocks, CAP), TOKENS, jnp.int32).at[route_blocks, block_ids, slot_ids].set(token_ids)
    padded = jnp.concatenate([normed, jnp.zeros((1, D), jnp.bfloat16)], 0)
    hidden_block = FF // N_TP

    def expert_work(expert_id):
        rows = padded[table[expert_id].reshape(-1)]
        gate_pre = jnp.dot(rows, expert_gate[expert_id], preferred_element_type=jnp.float32)
        up_pre = jnp.dot(rows, expert_up[expert_id], preferred_element_type=jnp.float32)
        glu_part = jnp.minimum(gate_pre, 7.0)
        lin_part = jnp.clip(up_pre, -7.0, 7.0)
        hidden = (glu_part * jax.nn.sigmoid(1.702 * glu_part) * (lin_part + 1.0)).astype(jnp.bfloat16)
        summed = jnp.zeros((rows.shape[0], D), jnp.float32)
        for part_index in range(N_TP):
            piece_sum = jnp.dot(hidden[:, part_index * hidden_block:(part_index + 1) * hidden_block], expert_down[expert_id][part_index * hidden_block:(part_index + 1) * hidden_block], preferred_element_type=jnp.float32)
            summed = summed + lax.optimization_barrier(piece_sum.astype(jnp.bfloat16)).astype(jnp.float32)
        return summed.astype(jnp.bfloat16).reshape(blocks, CAP, D)
    outputs = lax.map(expert_work, jnp.arange(EXPERTS, dtype=jnp.int32))
    picked = outputs[route_blocks, block_ids, slot_ids].astype(jnp.float32)
    weighted = picked * route_weights.reshape(blocks, sub_rows * TOP_K)[..., None].astype(jnp.float32)
    routed = lax.optimization_barrier(jnp.sum(weighted.reshape(TOKENS, TOP_K, D), 1))
    return (after_mix.astype(jnp.float32) + rms_norm(routed, gain_post)).astype(jnp.bfloat16)
```

```python
import functools
import jax
import jax.numpy as jnp
from jax import lax
from jax.experimental import pallas as pl
from jax.experimental.pallas import tpu as pltpu
from jax.sharding import PartitionSpec as P

HA = 4
DA = 128
DB = 64
LOG2E = 1.4426950408889634
JOINED = 4


def in_blocks(array, dim, devices):
    before, after = (array.shape[:dim], array.shape[dim + 1 :])
    return jnp.moveaxis(array.reshape(*before, devices, -1, *after), dim, 0)


def summed_on_arrival(array, axis, dim):
    devices = lax.axis_size(axis)
    blocks = lax.all_to_all(in_blocks(array, dim, devices), axis, 0, 0, tiled=True)
    return jnp.sum(blocks.astype(jnp.float32), axis=0)


def rms_norm(values, gain_vec):
    return values * lax.rsqrt(jnp.mean(values * values, -1, keepdims=True) + 1e-06) * gain_vec

def attn_kernel(n_units, n_sub, tile_rows, scale, slot_ref, lam_ref, q_ref, kv_ref, gain_ref, out_ref, m_ref, l_ref, acc_ref):
    t = pl.program_id(0)
    rows = q_ref.shape[2]
    slot = slot_ref[0]
    last = (slot * rows) // tile_rows
    heads = n_units // 2
    width = acc_ref.shape[1]
    blocks = tile_rows // rows

    @pl.when(t == 0)
    def _():
        m_ref[...] = jnp.full(m_ref.shape, -1e30, jnp.float32)
        l_ref[...] = jnp.zeros(l_ref.shape, jnp.float32)
        acc_ref[...] = jnp.zeros(acc_ref.shape, jnp.float32)

    def tile(masked):
        if masked:
            key_pos = t * tile_rows + lax.broadcasted_iota(jnp.int32, (tile_rows, rows), 0)
            query_pos = slot * rows + lax.broadcasted_iota(jnp.int32, (tile_rows, rows), 1)
            visible = key_pos <= query_pos
        for u in range(n_units):
            map_at, head = u // heads, u % heads
            keys = kv_ref[:, map_at * 128 : (map_at + 1) * 128]
            scores = jnp.dot(keys, q_ref[u], preferred_element_type=jnp.float32) * scale
            if masked:
                scores = jnp.where(visible, scores, -1e30)
            old = m_ref[u : u + 1]
            new = jnp.maximum(old, jnp.max(scores, axis=0, keepdims=True))
            terms = jnp.exp2(scores - new)
            shrink = jnp.exp2(old - new)
            m_ref[u : u + 1] = new
            l_ref[u : u + 1] = l_ref[u : u + 1] * shrink + jnp.sum(terms, axis=0, keepdims=True)
            terms = terms.astype(jnp.bfloat16)
            at = 256 + 0 * head
            vals = jnp.concatenate(
                [kv_ref[b * rows + head * width : b * rows + (head + 1) * width, at : at + rows] for b in range(blocks)],
                axis=1,
            )
            acc_ref[u] = acc_ref[u] * shrink + jnp.dot(vals, terms, preferred_element_type=jnp.float32)

    @pl.when(t < last)
    def _():
        tile(False)

    @pl.when(t == last)
    def _():
        tile(True)
        for head in range(heads):
            one, two = head, heads + head
            mix = acc_ref[one] / l_ref[one : one + 1] - lam_ref[head] * acc_ref[two] / l_ref[two : two + 1]
            mean = jnp.mean(mix * mix, axis=0, keepdims=True)
            normed = mix * lax.rsqrt(mean + 1e-6) * gain_ref[...]
            out_ref[:, head * width : (head + 1) * width] = normed.T.astype(jnp.bfloat16)


def attention(slot, lam, queries, kv, gain, head_size, tile_rows=512):
    rows, _, channels = queries.shape
    heads = channels // head_size
    width = 2 * head_size
    qt = jnp.transpose(queries, (1, 2, 0))
    keep = (jnp.arange(channels)[None, :] // head_size == jnp.arange(heads)[:, None])[None, :, :, None]
    units = jnp.where(keep, qt[:, None], jnp.zeros((), jnp.bfloat16)).reshape(2 * heads, channels, rows)
    keys = kv.shape[0]
    n_units = 2 * heads
    grid_spec = pltpu.PrefetchScalarGridSpec(
        num_scalar_prefetch=1,
        grid=(keys // tile_rows,),
        in_specs=[
            pl.BlockSpec(memory_space=pltpu.SMEM),
            pl.BlockSpec((n_units, channels, rows), lambda t, s: (0, 0, 0)),
            pl.BlockSpec((tile_rows, kv.shape[1]), lambda t, s: (jnp.minimum(t, (s[0] * rows) // tile_rows), 0)),
            pl.BlockSpec((width, 1), lambda t, s: (0, 0)),
        ],
        out_specs=pl.BlockSpec((rows, heads * width), lambda t, s: (0, 0)),
        scratch_shapes=[
            pltpu.VMEM((n_units, rows), jnp.float32),
            pltpu.VMEM((n_units, rows), jnp.float32),
            pltpu.VMEM((n_units, width, rows), jnp.float32),
        ],
    )
    flops = 2 * rows * keys * n_units * (channels + width) // 2
    return pl.pallas_call(
        functools.partial(attn_kernel, n_units, heads, tile_rows, head_size ** (-0.5) * LOG2E),
        grid_spec=grid_spec,
        out_shape=jax.ShapeDtypeStruct((rows, heads * width), jnp.bfloat16),
        cost_estimate=pl.CostEstimate(flops=flops, bytes_accessed=2 * keys * kv.shape[1], transcendentals=n_units * rows * keys),
        name="attend",
    )(slot.reshape(1), lam, units, kv, gain.reshape(width, 1))


def pack(keys, values):
    rows = keys.shape[0]
    return jnp.concatenate([keys.reshape(rows, -1), values.T], axis=1)


def ffn_kernel(x_ref, gate_ref, up_ref, down_ref, out_ref):
    x = x_ref[...]
    gate_pre = jnp.dot(x, gate_ref[0], preferred_element_type=jnp.float32)
    up_pre = jnp.dot(x, up_ref[0], preferred_element_type=jnp.float32)
    glu_part = jnp.minimum(gate_pre, 7.0)
    lin_part = jnp.clip(up_pre, -7.0, 7.0)
    hidden = (glu_part * jax.nn.sigmoid(1.702 * glu_part) * (lin_part + 1.0)).astype(jnp.bfloat16)
    out_ref[...] = jnp.dot(hidden, down_ref[0], preferred_element_type=jnp.float32).astype(jnp.bfloat16)


def ffn(x, gate, up, down, tile_rows):
    rows, width = x.shape
    hidden = gate.shape[2]
    return pl.pallas_call(
        ffn_kernel,
        grid=(rows // tile_rows,),
        in_specs=[
            pl.BlockSpec((tile_rows, width), lambda i: (i, 0)),
            pl.BlockSpec(gate.shape, lambda i: (0, 0, 0)),
            pl.BlockSpec(up.shape, lambda i: (0, 0, 0)),
            pl.BlockSpec(down.shape, lambda i: (0, 0, 0)),
        ],
        out_specs=pl.BlockSpec((tile_rows, width), lambda i: (i, 0)),
        out_shape=jax.ShapeDtypeStruct((rows, width), jnp.bfloat16),
        cost_estimate=pl.CostEstimate(
            flops=6 * rows * width * hidden, bytes_accessed=4 * rows * width + 6 * width * hidden, transcendentals=rows * hidden
        ),
        name="expert",
    )(x, gate, up, down)


def grouped_kernel(left_ref, right_ref, out_ref):
    out_ref[0] = jnp.dot(left_ref[0], right_ref[0], preferred_element_type=jnp.float32).astype(jnp.bfloat16)


def grouped_dot(left, right):
    groups, rows, depth = left.shape
    width = right.shape[2]
    return pl.pallas_call(
        grouped_kernel,
        grid=(groups,),
        in_specs=[
            pl.BlockSpec((1, rows, depth), lambda i: (i, 0, 0)),
            pl.BlockSpec((1, depth, width), lambda i: (i, 0, 0)),
        ],
        out_specs=pl.BlockSpec((1, rows, width), lambda i: (i, 0, 0)),
        out_shape=jax.ShapeDtypeStruct((groups, rows, width), jnp.bfloat16),
        cost_estimate=pl.CostEstimate(
            flops=2 * groups * rows * depth * width,
            bytes_accessed=2 * groups * (rows * depth + depth * width + rows * width),
            transcendentals=0,
        ),
        name="pick",
    )(left, right)


def slot_tables(info, top_count, expert, capacity, joined):
    sources, rows, _ = info.shape
    match = info[..., :top_count] == expert.astype(jnp.float32)
    hit = jnp.any(match, -1)
    weight = jnp.sum(jnp.where(match, info[..., top_count:], 0.0), -1)
    order = jnp.arange(rows)
    earlier = (order[None, :] < order[:, None])[None]
    before = jnp.sum(jnp.where(earlier & hit[:, None, :], 1, 0), -1)
    place = (jnp.arange(sources) % joined)[:, None] * capacity + before
    place = jnp.where(hit, place, -1).reshape(sources // joined, joined * rows)
    weight = weight.reshape(sources // joined, joined * rows)
    slots = jnp.arange(joined * capacity)
    picks = place[:, None, :] == slots[None, :, None]
    slot_weight = jnp.sum(jnp.where(picks, weight[:, None, :], 0.0), -1)
    puts = place[:, :, None] == slots[None, None, :]
    return picks.astype(jnp.bfloat16), puts.astype(jnp.bfloat16), slot_weight


def per_device(
    queries_a,
    keys_a,
    values_a,
    queries_b,
    keys_b,
    values_b,
    lambdas,
    head_gain_a,
    head_gain_b,
    out_a,
    out_b,
    residual,
    gain_mix,
    gain_pre,
    gain_post,
    routes,
    route_weights,
    expert_gate,
    expert_up,
    expert_down,
):
    heads_a = queries_a.shape[2] // DA
    heads_b = queries_b.shape[2] // DB
    head_slot = lax.axis_index("tp")
    seq_slot = lax.axis_index("sp")
    experts = lax.axis_size("sp")
    parts = lax.axis_size("tp")
    lambda_a = lax.dynamic_slice_in_dim(lambdas, head_slot * heads_a, heads_a)
    lambda_b = lax.dynamic_slice_in_dim(lambdas, HA + head_slot * heads_b, heads_b)
    sub_rows, width = residual.shape
    top_count = routes.shape[1]
    capacity = min(sub_rows, (5 * sub_rows * top_count + 4 * experts - 1) // (4 * experts))

    filled_a = lax.all_gather(pack(keys_a, values_a), "sp", axis=0, tiled=True)
    filled_b = lax.all_gather(pack(keys_b, values_b), "sp", axis=0, tiled=True)
    own_info = jnp.concatenate([routes.astype(jnp.float32), route_weights], axis=1)
    info = lax.all_gather(own_info, "sp", axis=0)
    picks, puts, slot_weight = slot_tables(info, top_count, seq_slot, capacity, JOINED)

    heads_out_a = attention(seq_slot, lambda_a, queries_a, filled_a, head_gain_a, DA)
    heads_out_b = attention(seq_slot, lambda_b, queries_b, filled_b, head_gain_b, DB)
    partial = (
        jnp.dot(heads_out_a, out_a, preferred_element_type=jnp.float32)
        + jnp.dot(heads_out_b, out_b, preferred_element_type=jnp.float32)
    ).astype(jnp.bfloat16)
    mixed_rows = summed_on_arrival(partial, "tp", 0)
    after_mix = (residual.astype(jnp.float32) + rms_norm(mixed_rows, gain_mix)).astype(jnp.bfloat16)
    normed = rms_norm(after_mix.astype(jnp.float32), gain_pre).astype(jnp.bfloat16)

    tokens = lax.all_gather(normed, "sp", axis=0, tiled=True)
    picked = grouped_dot(picks, tokens.reshape(experts // JOINED, JOINED * sub_rows, width))
    gathered = lax.all_gather(picked.reshape(-1, width), "tp", axis=0, tiled=True)
    partials = ffn(gathered, expert_gate, expert_up, expert_down, experts * capacity)
    mine = lax.psum_scatter(partials, "tp", scatter_dimension=0, tiled=True)
    scaled = (mine.astype(jnp.float32) * slot_weight.reshape(-1, 1)).astype(jnp.bfloat16)
    spread = grouped_dot(puts, scaled.reshape(experts // JOINED, JOINED * capacity, width))
    routed = lax.psum_scatter(spread.reshape(-1, width), "sp", scatter_dimension=0, tiled=True)
    routed = routed.astype(jnp.float32)
    return (after_mix.astype(jnp.float32) + rms_norm(routed, gain_post)).astype(jnp.bfloat16)


def solution(mesh):
    in_specs = (
        P(("grp", "sp"), None, "tp"),
        P(("grp", "sp"), None, "tp"),
        P(("grp", "sp"), "tp"),
        P(("grp", "sp"), None, "tp"),
        P(("grp", "sp"), None, "tp"),
        P(("grp", "sp"), "tp"),
        P(),
        P(),
        P(),
        P("tp", None),
        P("tp", None),
        P(("grp", "sp", "tp"), None),
        P(),
        P(),
        P(),
        P(("grp", "sp", "tp"), None),
        P(("grp", "sp", "tp"), None),
        P("sp", None, "tp"),
        P("sp", None, "tp"),
        P("sp", "tp", None),
    )
    out_specs = P(("grp", "sp", "tp"), None)
    return jax.shard_map(
        per_device, mesh=mesh, in_specs=in_specs, out_specs=out_specs, check_vma=False
    )
```

```python
import functools

import jax
import jax.numpy as jnp
from jax import lax
from jax.experimental import pallas as pl
from jax.experimental.pallas import tpu as pltpu
from jax.sharding import PartitionSpec as P

HA = 4
DA = 128
DB = 64
CORES = 2
JOINED = 4
LOG2E = 1.4426950408889634
ROOM = 40 * 1024 * 1024


def along(array, chips, step):
    pairs = [(z * CORES + c, (z + step) % chips * CORES + c) for z in range(chips) for c in range(CORES)]
    return lax.ppermute(array, "sp", pairs)


def across(array, chips):
    return lax.ppermute(array, "sp", [(i, i ^ 1) for i in range(chips * CORES)])


def sideways(array, parts, step):
    return lax.ppermute(array, "tp", [(i, (i + step) % parts) for i in range(parts)])


def in_blocks(array, dim, devices):
    before, after = (array.shape[:dim], array.shape[dim + 1 :])
    return jnp.moveaxis(array.reshape(*before, devices, -1, *after), dim, 0)


def summed_on_arrival(array, axis, dim):
    devices = lax.axis_size(axis)
    blocks = lax.all_to_all(in_blocks(array, dim, devices), axis, 0, 0, tiled=True)
    return jnp.sum(blocks.astype(jnp.float32), axis=0)


def rms_norm(values, gain_vec):
    return values * lax.rsqrt(jnp.mean(values * values, -1, keepdims=True) + 1e-06) * gain_vec


def whole(array):
    return pl.BlockSpec(array.shape, lambda *_: (0,) * array.ndim)


def params():
    return pltpu.CompilerParams(vmem_limit_bytes=ROOM)


def absorb(n_units, width, scale, q_ref, kv_ref, block, states, causal):
    heads = n_units // 2
    rows = kv_ref.shape[1]
    channels = q_ref.shape[1]

    @pl.loop(0, n_units)
    def _(u):
        lanes = pl.ds(pl.multiple_of((u // heads) * channels, channels), channels)
        keys = kv_ref[block, :, lanes]
        vals = kv_ref[block, pl.ds(pl.multiple_of((u % heads) * width, width), width), 2 * channels :]
        base = pl.multiple_of(u * (width + 16), 16)
        for at, state in states:
            scores = (
                jnp.dot(keys, q_ref[u, :, at * rows : (at + 1) * rows], preferred_element_type=jnp.float32) * scale
            )
            if causal:
                key_pos = lax.broadcasted_iota(jnp.int32, scores.shape, 0)
                query_pos = lax.broadcasted_iota(jnp.int32, scores.shape, 1)
                scores = jnp.where(key_pos <= query_pos, scores, -1e30)
            top_rows, total_rows = pl.ds(base + width, 8), pl.ds(base + width + 8, 8)
            old = state[top_rows]
            new = jnp.maximum(old, jnp.max(scores, axis=0, keepdims=True))
            terms = jnp.exp2(scores - new[:1])
            shrink = jnp.exp2(old - new)
            state[top_rows] = new
            state[total_rows] = state[total_rows] * shrink + jnp.sum(terms, axis=0, keepdims=True)
            place = pl.ds(base, width)
            state[place] = state[place] * shrink[:1] + jnp.dot(
                vals, terms.astype(jnp.bfloat16), preferred_element_type=jnp.float32
            )


def first_kernel(n_units, width, scale, flags, q_ref, kv_ref, own_ref, other_ref):
    for u in range(n_units):
        base = u * (width + 16)
        for state in (own_ref, other_ref):
            state[base : base + width + 16] = jnp.zeros((width + 16, state.shape[1]), jnp.float32)
            state[base + width : base + width + 8] = jnp.full((8, state.shape[1]), -1e30, jnp.float32)
    absorb(n_units, width, scale, q_ref, kv_ref, 0, ((0, own_ref),), True)

    @pl.when(flags[0] > 0)
    def _():
        absorb(n_units, width, scale, q_ref, kv_ref, 0, ((1, other_ref),), False)


def step_kernel(n_units, width, scale, n_blocks, flags, q_ref, own_in, other_in, *refs):
    blocks, (own_ref, other_ref, kv_ref) = refs[:n_blocks], refs[n_blocks:]
    own_ref[...] = own_in[...]
    other_ref[...] = other_in[...]
    for i in range(n_blocks):
        kv_ref[i] = blocks[i][...]

    @pl.loop(0, n_blocks)
    def _(i):
        @pl.when(flags[i] > 0)
        def _():
            absorb(n_units, width, scale, q_ref, kv_ref, i, ((0, own_ref), (1, other_ref)), False)


def attend(units, head_size, flags, state, blocks):
    n_units, channels, both = units.shape
    width = 2 * head_size
    rows = both // 2
    scale = head_size ** (-0.5) * LOG2E
    shape = jax.ShapeDtypeStruct((n_units * (width + 16), rows), jnp.float32)
    if state is None:
        kernel = functools.partial(first_kernel, n_units, width, scale)
        operands = (units, blocks[0][None])
        scratch = []
    else:
        kernel = functools.partial(step_kernel, n_units, width, scale, len(blocks))
        operands = (units, *state, *blocks)
        scratch = [pltpu.VMEM((len(blocks), *blocks[0].shape), jnp.bfloat16)]
    spec = pl.BlockSpec(shape.shape, lambda *_: (0, 0))
    work = len(blocks) * rows * both * n_units
    return pl.pallas_call(
        kernel,
        grid_spec=pltpu.PrefetchScalarGridSpec(
            num_scalar_prefetch=1,
            grid=(1,),
            in_specs=[whole(a) for a in operands],
            out_specs=[spec, spec],
            scratch_shapes=scratch,
        ),
        out_shape=[shape, shape],
        input_output_aliases={} if state is None else {2: 0, 3: 1},
        cost_estimate=pl.CostEstimate(
            flops=4 * work * (channels + width), bytes_accessed=6 * shape.size * 4, transcendentals=work
        ),
        compiler_params=params(),
        name="attend",
    )(flags, *operands)


def merge_kernel(sizes, lam_a, lam_b, own_a, got_a, own_b, got_b, gain_a, gain_b, proj_a, proj_b, *refs):
    out_ref = refs[-1]
    result = None
    groups = ((lam_a, own_a, got_a, gain_a, proj_a), (lam_b, own_b, got_b, gain_b, proj_b))
    for (heads, width), (lam, own, got, gain, proj) in zip(sizes, groups):

        def share(u):
            base = u * (width + 16)
            at = base + width
            one, two = own[at : at + 1], got[at : at + 1]
            top = jnp.maximum(one, two)
            one, two = jnp.exp2(one - top), jnp.exp2(two - top)
            at = at + 8
            total = own[at : at + 1] * one + got[at : at + 1] * two
            place = slice(base, base + width)
            return (own[place] * one + got[place] * two) / total

        for head in range(heads):
            mix = share(head) - lam[head] * share(heads + head)
            mean = jnp.mean(mix * mix, axis=0, keepdims=True)
            normed = (mix * lax.rsqrt(mean + 1e-6) * gain[...]).T.astype(jnp.bfloat16)
            part = jnp.dot(normed, proj[head * width : (head + 1) * width], preferred_element_type=jnp.float32)
            result = part if result is None else result + part
    out_ref[...] = result.astype(jnp.bfloat16)


def merge(sizes, lam_a, lam_b, own_a, got_a, own_b, got_b, gain_a, gain_b, proj_a, proj_b, tables):
    rows = own_a.shape[1]
    operands = (own_a, got_a, own_b, got_b, gain_a.reshape(-1, 1), gain_b.reshape(-1, 1), proj_a, proj_b)
    out = jax.ShapeDtypeStruct((rows, proj_a.shape[1]), jnp.bfloat16)
    return pl.pallas_call(
        functools.partial(merge_kernel, sizes),
        grid=(1,),
        in_specs=[pl.BlockSpec(memory_space=pltpu.SMEM)] * 2
        + [whole(a) for a in operands]
        + [pl.BlockSpec(memory_space=pl.ANY)] * len(tables),
        out_specs=pl.BlockSpec(out.shape, lambda i: (0, 0)),
        out_shape=out,
        cost_estimate=pl.CostEstimate(
            flops=4 * rows * proj_a.size, bytes_accessed=8 * proj_a.size, transcendentals=0
        ),
        compiler_params=params(),
        name="merge",
    )(lam_a, lam_b, *operands, *tables)


def stacked(refs):
    return jnp.concatenate([r[...].astype(jnp.float32) for r in refs], axis=0).astype(jnp.bfloat16)


def ffn_kernel(count, tile, gate_ref, up_ref, down_ref, *refs):
    ins, outs, (rows_ref, sum_ref) = refs[:count], refs[count : 2 * count], refs[-2:]
    half = pl.program_id(0)
    each = ins[0].shape[0]
    together = tile // each

    @pl.when(half == 0)
    def _():
        for i in range(0, count, together):
            rows_ref[i * each : i * each + tile] = stacked(ins[i : i + together])

    @pl.loop(0, count // together)
    def _(i):
        place = pl.ds(pl.multiple_of(i * tile, tile), tile)
        x = rows_ref[place]
        gate_pre = jnp.dot(x, gate_ref[0], preferred_element_type=jnp.float32)
        up_pre = jnp.dot(x, up_ref[0], preferred_element_type=jnp.float32)
        glu_part = jnp.minimum(gate_pre, 7.0)
        lin_part = jnp.clip(up_pre, -7.0, 7.0)
        hidden = (glu_part * jax.nn.sigmoid(1.702 * glu_part) * (lin_part + 1.0)).astype(jnp.bfloat16)
        part = jnp.dot(hidden, down_ref[0], preferred_element_type=jnp.float32)

        @pl.when(half == 0)
        def _():
            sum_ref[place] = part

        @pl.when(half == 1)
        def _():
            sum_ref[place] = sum_ref[place] + part

    @pl.when(half == 1)
    def _():
        for i in range(count):
            outs[i][...] = sum_ref[i * each : (i + 1) * each].astype(jnp.bfloat16)


def ffn(groups, gate, up, down, after):
    arrays = [a for group in groups for a in group]
    count = len(arrays)
    each, width = arrays[0].shape
    hidden = gate.shape[2]
    per = hidden // 2
    rows = each * count

    def kernel(*refs):
        ffn_kernel(count, each * 8, *refs[:3], *refs[4:])

    out = pl.pallas_call(
        kernel,
        grid=(2,),
        in_specs=[
            pl.BlockSpec((1, width, per), lambda i: (0, 0, i)),
            pl.BlockSpec((1, width, per), lambda i: (0, 0, i)),
            pl.BlockSpec((1, per, width), lambda i: (0, i, 0)),
            pl.BlockSpec(memory_space=pl.ANY),
        ]
        + [whole(a) for a in arrays],
        out_specs=[whole(a) for a in arrays],
        out_shape=[jax.ShapeDtypeStruct(a.shape, jnp.bfloat16) for a in arrays],
        scratch_shapes=[pltpu.VMEM((rows, width), jnp.bfloat16), pltpu.VMEM((rows, width), jnp.float32)],
        cost_estimate=pl.CostEstimate(
            flops=6 * rows * width * hidden, bytes_accessed=4 * rows * width + 6 * width * hidden, transcendentals=rows * hidden
        ),
        compiler_params=pltpu.CompilerParams(vmem_limit_bytes=56 * 1024 * 1024),
        name="expert",
    )(gate, up, down, after, *arrays)
    return [out[i : i + 8] for i in range(0, count, 8)]


def pick_kernel(picks_ref, *refs):
    outs = refs[-2:]
    for part in range(2):
        rows = jnp.concatenate([r[...] for r in refs[part:-2:2]], axis=0)
        cols = slice(part * rows.shape[1], (part + 1) * rows.shape[1])
        for p in range(2):
            outs[p][:, cols] = jnp.dot(picks_ref[p, 0], rows, preferred_element_type=jnp.float32).astype(jnp.bfloat16)


def pick(picks, group, sources):
    arrays = [a for pair in sources for a in pair]
    slots = picks.shape[2]
    width = 2 * arrays[0].shape[1]
    out = jax.ShapeDtypeStruct((slots, width), jnp.bfloat16)
    spec = pl.BlockSpec(out.shape, lambda i: (0, 0))
    return pl.pallas_call(
        pick_kernel,
        grid=(1,),
        in_specs=[pl.BlockSpec((2, 1, *picks.shape[2:]), lambda i: (0, group, 0, 0))] + [whole(a) for a in arrays],
        out_specs=[spec, spec],
        out_shape=[out, out],
        cost_estimate=pl.CostEstimate(
            flops=4 * slots * picks.shape[3] * width, bytes_accessed=4 * picks.shape[3] * width, transcendentals=0
        ),
        compiler_params=params(),
        name="pick",
    )(picks, *arrays)


def spread_kernel(puts_ref, weight_ref, *refs):
    ins, outs = refs[:4], refs[4:]
    own = sum(r[...].astype(jnp.float32) for r in ins[:3]) * weight_ref[0, 0]
    other = ins[3][...].astype(jnp.float32) * weight_ref[1, 0]
    slots = jnp.concatenate([own, other], axis=0).astype(jnp.bfloat16)
    rows, cols = outs[0].shape
    for i in range(len(outs) // 2):
        for part in range(2):
            outs[2 * i + part][...] = jnp.dot(
                puts_ref[0, i * rows : (i + 1) * rows],
                slots[:, part * cols : (part + 1) * cols],
                preferred_element_type=jnp.float32,
            ).astype(jnp.bfloat16)


def spread(puts, weights, group, own, other):
    arrays = (*own, other)
    slots, width = other.shape
    rows = puts.shape[1] // JOINED
    out = jax.ShapeDtypeStruct((rows, width // 2), jnp.bfloat16)
    spec = pl.BlockSpec(out.shape, lambda i: (0, 0))
    count = 2 * JOINED
    flat = pl.pallas_call(
        spread_kernel,
        grid=(1,),
        in_specs=[
            pl.BlockSpec((1, *puts.shape[1:]), lambda i: (group, 0, 0)),
            pl.BlockSpec((2, 1, slots, 1), lambda i: (0, group, 0, 0)),
        ]
        + [whole(a) for a in arrays],
        out_specs=[spec] * count,
        out_shape=[out] * count,
        cost_estimate=pl.CostEstimate(
            flops=4 * puts.shape[1] * slots * width, bytes_accessed=4 * puts.shape[1] * width, transcendentals=0
        ),
        compiler_params=params(),
        name="spread",
    )(puts, weights, *arrays)
    return [(flat[2 * i], flat[2 * i + 1]) for i in range(JOINED)]


def slot_tables(info, top_count, expert, capacity):
    sources, _, rows = info.shape
    wanted = jnp.stack([expert, expert ^ 1]).astype(jnp.float32)[:, None, None, None]
    match = info[None, :, :top_count] == wanted
    hit = jnp.any(match, 2)
    weight = jnp.sum(jnp.where(match, info[None, :, top_count:], 0.0), 2)
    order = jnp.arange(rows)
    before = jnp.dot(
        hit.astype(jnp.bfloat16).reshape(2 * sources, rows),
        (order[:, None] < order[None, :]).astype(jnp.bfloat16),
        preferred_element_type=jnp.float32,
    ).reshape(2, sources, rows)
    offset = ((jnp.arange(sources) % JOINED) * capacity)[None, :, None]
    place = jnp.where(hit, before.astype(jnp.int32) + offset, -1)
    groups = sources // JOINED
    place = place.reshape(2, groups, JOINED * rows)
    weight = weight.reshape(2, groups, 1, JOINED * rows)
    slots = jnp.arange(JOINED * capacity)
    picks = place[:, :, None, :] == slots[None, None, :, None]
    slot_weight = jnp.sum(jnp.where(picks, weight, 0.0), -1, keepdims=True)
    puts = place[:, :, :, None] == slots
    puts = jnp.concatenate([puts[0], puts[1]], axis=-1)
    return picks.astype(jnp.bfloat16), puts.astype(jnp.bfloat16), slot_weight


def query_units(queries, head_size, chips):
    rows, _, channels = queries.shape
    heads = channels // head_size
    own = jnp.transpose(queries, (1, 2, 0))
    both = jnp.concatenate([own, across(own, chips)], axis=2)
    keep = (jnp.arange(channels)[None, :] // head_size == jnp.arange(heads)[:, None])[None, :, :, None]
    return jnp.where(keep, both[:, None], jnp.zeros((), jnp.bfloat16)).reshape(2 * heads, channels, 2 * rows)


def pack(keys, values):
    rows = keys.shape[0]
    return jnp.concatenate([keys.reshape(rows, -1), values.T], axis=1)


def added(one, two):
    return (one.astype(jnp.float32) + two.astype(jnp.float32)).astype(jnp.bfloat16)


def gather_columns(own, got, parts):
    f_own, f_got = sideways(own, parts, 1), sideways(got, parts, 1)
    g_own, g_got = sideways(own, parts, -1), sideways(got, parts, -1)
    far_own, far_got = sideways(f_own, parts, 1), sideways(g_got, parts, -1)
    return [own, got, f_own, f_got, g_own, g_got, far_own, far_got]


def return_columns(done, parts, later):
    own, got, f_own, f_got, g_own, g_got, far_own, far_got = done
    u, v = sideways(far_own, parts, -1), sideways(far_got, parts, 1)
    w_got, x_own = sideways(f_got, parts, -1), sideways(g_own, parts, 1)
    sum_own, sum_got = added(f_own, u), added(g_got, v)
    if later is not None:
        (sum_own, sum_got), later = lax.optimization_barrier(((sum_own, sum_got), later))
    w_own, x_got = sideways(sum_own, parts, -1), sideways(sum_got, parts, 1)
    total = got.astype(jnp.float32) + w_got.astype(jnp.float32) + x_got.astype(jnp.float32)
    return (own, w_own, x_own), total.astype(jnp.bfloat16), later


def per_device(
    queries_a,
    keys_a,
    values_a,
    queries_b,
    keys_b,
    values_b,
    lambdas,
    head_gain_a,
    head_gain_b,
    out_a,
    out_b,
    residual,
    gain_mix,
    gain_pre,
    gain_post,
    routes,
    route_weights,
    expert_gate,
    expert_up,
    expert_down,
):
    heads_a = queries_a.shape[2] // DA
    heads_b = queries_b.shape[2] // DB
    head_slot = lax.axis_index("tp")
    seq_slot = lax.axis_index("sp")
    experts = lax.axis_size("sp")
    parts = lax.axis_size("tp")
    chips = experts // CORES
    half = chips // 2
    chip, core = seq_slot // CORES, seq_slot % CORES
    lambda_a = lax.dynamic_slice_in_dim(lambdas, head_slot * heads_a, heads_a)
    lambda_b = lax.dynamic_slice_in_dim(lambdas, HA + head_slot * heads_b, heads_b)
    sub_rows, width = residual.shape
    top_count = routes.shape[1]
    capacity = min(sub_rows, (5 * sub_rows * top_count + 4 * experts - 1) // (4 * experts))

    blocks = [pack(keys_a, values_a), pack(keys_b, values_b)]
    units = [query_units(queries_a, DA, chips), query_units(queries_b, DB, chips)]
    sizes = (DA, DB)
    first_flag = jnp.where(core == 0, 1, 0).astype(jnp.int32).reshape(1)
    states = [attend(units[i], sizes[i], first_flag, None, blocks[i : i + 1]) for i in range(2)]
    ahead, behind = list(blocks), list(blocks)
    for step in range(1, half + 1):
        seen_ahead = (chip >= step).astype(jnp.int32)
        seen_behind = (chip + step >= chips).astype(jnp.int32)
        for i in range(2):
            use, flags = [], []
            if step < half or i == 0:
                ahead[i] = along(ahead[i], chips, 1)
                use.append(ahead[i])
                flags.append(seen_ahead)
            if step < half or i == 1:
                behind[i] = along(behind[i], chips, -1)
                use.append(behind[i])
                flags.append(seen_behind)
            states[i] = attend(units[i], sizes[i], jnp.stack(flags), states[i], use)

    own_info = jnp.concatenate([routes.astype(jnp.float32), route_weights], axis=1).T
    source_steps = [0] + [s for d in range(1, half) for s in (d, -d)] + [half]
    info = jnp.stack([own_info if s == 0 else along(own_info, chips, s) for s in source_steps])
    picks, puts, slot_weight = slot_tables(info, top_count, seq_slot, capacity)

    got = [across(states[i][1], chips) for i in range(2)]
    partial = merge(
        ((heads_a, 2 * DA), (heads_b, 2 * DB)),
        lambda_a, lambda_b, states[0][0], got[0], states[1][0], got[1], head_gain_a, head_gain_b, out_a, out_b,
        (picks, puts, slot_weight),
    )
    mixed_rows = summed_on_arrival(partial, "tp", 0)
    after_mix = (residual.astype(jnp.float32) + rms_norm(mixed_rows, gain_mix)).astype(jnp.bfloat16)
    normed = rms_norm(after_mix.astype(jnp.float32), gain_pre).astype(jnp.bfloat16)

    ahead = [normed[:, : width // 2], normed[:, width // 2 :]]
    behind = list(ahead)
    sources = [tuple(ahead)]
    columns = []

    def hold(*values):
        held, values = lax.optimization_barrier((tuple(ahead), values))
        ahead[:] = held
        return values

    def pick_group():
        k = len(columns)
        rows = pick(picks, k, sources[k * JOINED : (k + 1) * JOINED])
        (rows,) = hold(rows)
        columns.append(gather_columns(rows[0], across(rows[1], chips), parts))

    picked_at = []
    for step in range(1, half + 1):
        for i in range(2):
            if step < half or i == 0:
                ahead[i] = along(ahead[i], chips, 1)
            if step < half or i == 1:
                behind[i] = along(behind[i], chips, -1)
        if len(sources) >= (len(columns) + 1) * JOINED:
            pick_group()
            picked_at.append(step)
        for k, since in enumerate(picked_at):
            if step == since + 3:
                (columns[k][:6],) = hold(columns[k][:6])
            if step == since + 4:
                (columns[k][6:],) = hold(columns[k][6:])
        sources += [tuple(ahead), tuple(behind)] if step < half else [(ahead[0], behind[1])]
    pick_group()
    groups = len(columns)
    last = columns[-1]
    done = []
    after = last[0]
    if groups > 1:
        done = ffn(columns[:-1], expert_gate, expert_up, expert_down, after)
        after = done[-1][0]
    done = done + ffn([last], expert_gate, expert_up, expert_down, after)

    shares = {}
    for k in reversed(range(groups)):
        own_parts, other_sum, later = return_columns(done[k], parts, done[k - 1] if k else None)
        if k:
            done[k - 1] = later
        pairs = spread(puts, slot_weight, k, own_parts, across(other_sum, chips))
        for s, pair in zip(source_steps[k * JOINED : (k + 1) * JOINED], pairs):
            shares[s] = pair
    final = []
    for i in range(2):
        total = shares[0][i].astype(jnp.float32)
        for sign, reach in ((1, half - i), (-1, half - 1 + i)):
            carried = None
            for distance in range(reach, 0, -1):
                part = shares[half if distance == half else sign * distance][i]
                carried = along(part if carried is None else added(carried, part), chips, -sign)
            total = total + carried.astype(jnp.float32)
        final.append(total)
    routed = jnp.concatenate(final, axis=1)
    return (after_mix.astype(jnp.float32) + rms_norm(routed, gain_post)).astype(jnp.bfloat16)


def solution(mesh):
    in_specs = (
        P(("grp", "sp"), None, "tp"),
        P(("grp", "sp"), None, "tp"),
        P(("grp", "sp"), "tp"),
        P(("grp", "sp"), None, "tp"),
        P(("grp", "sp"), None, "tp"),
        P(("grp", "sp"), "tp"),
        P(),
        P(),
        P(),
        P("tp", None),
        P("tp", None),
        P(("grp", "sp", "tp"), None),
        P(),
        P(),
        P(),
        P(("grp", "sp", "tp"), None),
        P(("grp", "sp", "tp"), None),
        P("sp", None, "tp"),
        P("sp", None, "tp"),
        P("sp", "tp", None),
    )
    out_specs = P(("grp", "sp", "tp"), None)
    return jax.shard_map(
        per_device, mesh=mesh, in_specs=in_specs, out_specs=out_specs, check_vma=False
    )
```

```python
import functools

import jax
import jax.numpy as jnp
from jax import lax
from jax.experimental import pallas as pl
from jax.experimental.pallas import tpu as pltpu
from jax.sharding import PartitionSpec as P

HA = 4
DA = 128
DB = 64
CORES = 2
JOINED = 8
LOG2E = 1.4426950408889634
ROOM = 40 * 1024 * 1024


def along(array, chips, step):
    pairs = [(z * CORES + c, (z + step) % chips * CORES + c) for z in range(chips) for c in range(CORES)]
    return lax.ppermute(array, "sp", pairs)


def across(array, chips):
    return lax.ppermute(array, "sp", [(i, i ^ 1) for i in range(chips * CORES)])


def sideways(array, parts, step):
    return lax.ppermute(array, "tp", [(i, (i + step) % parts) for i in range(parts)])


def in_blocks(array, dim, devices):
    before, after = (array.shape[:dim], array.shape[dim + 1 :])
    return jnp.moveaxis(array.reshape(*before, devices, -1, *after), dim, 0)


def summed_on_arrival(array, axis, dim):
    devices = lax.axis_size(axis)
    blocks = lax.all_to_all(in_blocks(array, dim, devices), axis, 0, 0, tiled=True)
    return jnp.sum(blocks.astype(jnp.float32), axis=0)


def rms_norm(values, gain_vec):
    return values * lax.rsqrt(jnp.mean(values * values, -1, keepdims=True) + 1e-06) * gain_vec


def whole(array):
    return pl.BlockSpec(array.shape, lambda *_: (0,) * array.ndim)


def params():
    return pltpu.CompilerParams(vmem_limit_bytes=ROOM)


def absorb(n_units, width, scale, q_ref, kv_ref, block, states, causal):
    heads = n_units // 2
    channels = q_ref.shape[1]
    rows = states[0][1].shape[1]

    @pl.loop(0, heads)
    def _(head):
        vals = kv_ref[block, pl.ds(pl.multiple_of(head * width, width), width), 2 * channels :]
        work = []
        for map_at in range(2):
            keys = kv_ref[block, :rows, map_at * channels : (map_at + 1) * channels]
            u = map_at * heads + head
            base = pl.multiple_of(u * (width + 16), 16)
            for at, state in states:
                scores = (
                    jnp.dot(keys, q_ref[u, :, at * rows : (at + 1) * rows], preferred_element_type=jnp.float32) * scale
                )
                if causal:
                    key_pos = lax.broadcasted_iota(jnp.int32, scores.shape, 0)
                    query_pos = lax.broadcasted_iota(jnp.int32, scores.shape, 1)
                    scores = jnp.where(key_pos <= query_pos, scores, -1e30)
                old, total = state[pl.ds(base + width, 8)], state[pl.ds(base + width + 8, 8)]
                new = jnp.maximum(old, jnp.max(scores, axis=0, keepdims=True))
                terms = jnp.exp2(scores - new[:1])
                shrink = jnp.exp2(old - new)
                total = total * shrink + jnp.sum(terms, axis=0, keepdims=True)
                part = jnp.dot(vals, terms.astype(jnp.bfloat16), preferred_element_type=jnp.float32)
                work.append((state, base, new, total, shrink, part))
        for state, base, new, total, shrink, part in work:
            place = pl.ds(base, width)
            state[place] = state[place] * shrink[:1] + part
            state[pl.ds(base + width, 8)] = new
            state[pl.ds(base + width + 8, 8)] = total


def first_kernel(n_units, width, scale, flags, q_ref, kv_ref, own_ref, other_ref):
    for u in range(n_units):
        base = u * (width + 16)
        for state in (own_ref, other_ref):
            state[base : base + width + 16] = jnp.zeros((width + 16, state.shape[1]), jnp.float32)
            state[base + width : base + width + 8] = jnp.full((8, state.shape[1]), -1e30, jnp.float32)
    absorb(n_units, width, scale, q_ref, kv_ref, 0, ((0, own_ref),), True)

    @pl.when(flags[0] > 0)
    def _():
        absorb(n_units, width, scale, q_ref, kv_ref, 0, ((1, other_ref),), False)


def step_kernel(n_units, width, scale, n_blocks, flags, q_ref, own_in, other_in, *refs):
    blocks, (own_ref, other_ref, kv_ref) = refs[:n_blocks], refs[n_blocks:]
    own_ref[...] = own_in[...]
    other_ref[...] = other_in[...]
    for i in range(n_blocks):
        kv_ref[i] = blocks[i][...]

    @pl.loop(0, n_blocks)
    def _(i):
        @pl.when(flags[i] > 0)
        def _():
            absorb(n_units, width, scale, q_ref, kv_ref, i, ((0, own_ref), (1, other_ref)), False)


def attend(units, head_size, flags, state, blocks):
    n_units, channels, both = units.shape
    width = 2 * head_size
    rows = both // 2
    scale = head_size ** (-0.5) * LOG2E
    shape = jax.ShapeDtypeStruct((n_units * (width + 16), rows), jnp.float32)
    if state is None:
        kernel = functools.partial(first_kernel, n_units, width, scale)
        operands = (units, blocks[0][None])
        scratch = []
    else:
        kernel = functools.partial(step_kernel, n_units, width, scale, len(blocks))
        operands = (units, *state, *blocks)
        scratch = [pltpu.VMEM((len(blocks), *blocks[0].shape), jnp.bfloat16)]
    spec = pl.BlockSpec(shape.shape, lambda *_: (0, 0))
    work = len(blocks) * rows * both * n_units
    return pl.pallas_call(
        kernel,
        grid_spec=pltpu.PrefetchScalarGridSpec(
            num_scalar_prefetch=1,
            grid=(1,),
            in_specs=[whole(a) for a in operands],
            out_specs=[spec, spec],
            scratch_shapes=scratch,
        ),
        out_shape=[shape, shape],
        input_output_aliases={} if state is None else {2: 0, 3: 1},
        cost_estimate=pl.CostEstimate(
            flops=4 * work * (channels + width), bytes_accessed=6 * shape.size * 4, transcendentals=work
        ),
        compiler_params=params(),
        name="attend",
    )(flags, *operands)


def merge_kernel(sizes, lam_a, lam_b, own_a, got_a, own_b, got_b, gain_a, gain_b, proj_a, proj_b, out_ref):
    result = None
    groups = ((lam_a, own_a, got_a, gain_a, proj_a), (lam_b, own_b, got_b, gain_b, proj_b))
    for (heads, width), (lam, own, got, gain, proj) in zip(sizes, groups):

        def share(u):
            base = u * (width + 16)
            at = base + width
            one, two = own[at : at + 1], got[at : at + 1]
            top = jnp.maximum(one, two)
            one, two = jnp.exp2(one - top), jnp.exp2(two - top)
            at = at + 8
            total = own[at : at + 1] * one + got[at : at + 1] * two
            place = slice(base, base + width)
            return (own[place] * one + got[place] * two) / total

        for head in range(heads):
            mix = share(head) - lam[head] * share(heads + head)
            mean = jnp.mean(mix * mix, axis=0, keepdims=True)
            normed = (mix * lax.rsqrt(mean + 1e-6) * gain[...]).T.astype(jnp.bfloat16)
            part = jnp.dot(normed, proj[head * width : (head + 1) * width], preferred_element_type=jnp.float32)
            result = part if result is None else result + part
    out_ref[...] = result.astype(jnp.bfloat16)


def merge(sizes, lam_a, lam_b, own_a, got_a, own_b, got_b, gain_a, gain_b, proj_a, proj_b):
    rows = own_a.shape[1]
    operands = (own_a, got_a, own_b, got_b, gain_a.reshape(-1, 1), gain_b.reshape(-1, 1), proj_a, proj_b)
    out = jax.ShapeDtypeStruct((rows, proj_a.shape[1]), jnp.bfloat16)
    return pl.pallas_call(
        functools.partial(merge_kernel, sizes),
        grid=(1,),
        in_specs=[pl.BlockSpec(memory_space=pltpu.SMEM)] * 2 + [whole(a) for a in operands],
        out_specs=pl.BlockSpec(out.shape, lambda i: (0, 0)),
        out_shape=out,
        cost_estimate=pl.CostEstimate(
            flops=4 * rows * proj_a.size, bytes_accessed=8 * proj_a.size, transcendentals=0
        ),
        compiler_params=params(),
        name="merge",
    )(lam_a, lam_b, *operands)


def stacked(refs):
    return jnp.concatenate([r[...].astype(jnp.float32) for r in refs], axis=0).astype(jnp.bfloat16)


def ffn_kernel(count, tile, gate_ref, up_ref, down_ref, *refs):
    ins, outs, (rows_ref, sum_ref) = refs[:count], refs[count : 2 * count], refs[-2:]
    half = pl.program_id(0)
    each = ins[0].shape[0]
    together = tile // each

    @pl.when(half == 0)
    def _():
        for i in range(0, count, together):
            rows_ref[i * each : i * each + tile] = stacked(ins[i : i + together])

    @pl.loop(0, count // together)
    def _(i):
        place = pl.ds(pl.multiple_of(i * tile, tile), tile)
        x = rows_ref[place]
        gate_pre = jnp.dot(x, gate_ref[0], preferred_element_type=jnp.float32)
        up_pre = jnp.dot(x, up_ref[0], preferred_element_type=jnp.float32)
        glu_part = jnp.minimum(gate_pre, 7.0)
        lin_part = jnp.clip(up_pre, -7.0, 7.0)
        hidden = (glu_part * jax.nn.sigmoid(1.702 * glu_part) * (lin_part + 1.0)).astype(jnp.bfloat16)
        part = jnp.dot(hidden, down_ref[0], preferred_element_type=jnp.float32)

        @pl.when(half == 0)
        def _():
            sum_ref[place] = part

        @pl.when(half == 1)
        def _():
            sum_ref[place] = sum_ref[place] + part

    @pl.when(half == 1)
    def _():
        for i in range(count):
            outs[i][...] = sum_ref[i * each : (i + 1) * each].astype(jnp.bfloat16)


def ffn(groups, gate, up, down, after):
    arrays = [a for group in groups for a in group]
    count = len(arrays)
    each, width = arrays[0].shape
    hidden = gate.shape[2]
    per = hidden // 2
    rows = each * count

    def kernel(*refs):
        ffn_kernel(count, each * 4, *refs[:3], *refs[4:])

    out = pl.pallas_call(
        kernel,
        grid=(2,),
        in_specs=[
            pl.BlockSpec((1, width, per), lambda i: (0, 0, i)),
            pl.BlockSpec((1, width, per), lambda i: (0, 0, i)),
            pl.BlockSpec((1, per, width), lambda i: (0, i, 0)),
            pl.BlockSpec(memory_space=pl.ANY),
        ]
        + [whole(a) for a in arrays],
        out_specs=[whole(a) for a in arrays],
        out_shape=[jax.ShapeDtypeStruct(a.shape, jnp.bfloat16) for a in arrays],
        scratch_shapes=[pltpu.VMEM((rows, width), jnp.bfloat16), pltpu.VMEM((rows, width), jnp.float32)],
        cost_estimate=pl.CostEstimate(
            flops=6 * rows * width * hidden, bytes_accessed=4 * rows * width + 6 * width * hidden, transcendentals=rows * hidden
        ),
        compiler_params=pltpu.CompilerParams(vmem_limit_bytes=56 * 1024 * 1024),
        name="expert",
    )(gate, up, down, after, *arrays)
    return [out[i : i + 8] for i in range(0, count, 8)]


def pick_kernel(counts, picks_ref, *refs):
    outs, at, rows = refs[-2:], 0, []
    for count in counts:
        pieces = [r[...] for r in refs[at : at + count]]
        rows.append(pieces[0] if count == 1 else jnp.concatenate(pieces, axis=1))
        at += count
    rows = jnp.concatenate(rows, axis=0)
    for p in range(2):
        outs[p][...] = jnp.dot(picks_ref[p, 0], rows, preferred_element_type=jnp.float32).astype(jnp.bfloat16)


def pick(picks, group, sources):
    arrays = [a for pieces in sources for a in pieces]
    slots = picks.shape[2]
    width = sum(a.shape[1] for a in sources[0])
    out = jax.ShapeDtypeStruct((slots, width), jnp.bfloat16)
    spec = pl.BlockSpec(out.shape, lambda i: (0, 0))
    return pl.pallas_call(
        functools.partial(pick_kernel, [len(pieces) for pieces in sources]),
        grid=(1,),
        in_specs=[pl.BlockSpec((2, 1, *picks.shape[2:]), lambda i: (0, group, 0, 0))] + [whole(a) for a in arrays],
        out_specs=[spec, spec],
        out_shape=[out, out],
        cost_estimate=pl.CostEstimate(
            flops=4 * slots * picks.shape[3] * width, bytes_accessed=4 * picks.shape[3] * width, transcendentals=0
        ),
        compiler_params=params(),
        name="pick",
    )(picks, *arrays)


def spread_kernel(puts_ref, weight_ref, *refs):
    ins, outs = refs[:4], refs[4:]
    own = sum(r[...].astype(jnp.float32) for r in ins[:3]) * weight_ref[0, 0]
    other = ins[3][...].astype(jnp.float32) * weight_ref[1, 0]
    slots = jnp.concatenate([own, other], axis=0).astype(jnp.bfloat16)
    rows, cols = outs[0].shape
    for i in range(len(outs) // 2):
        for part in range(2):
            outs[2 * i + part][...] = jnp.dot(
                puts_ref[0, i * rows : (i + 1) * rows],
                slots[:, part * cols : (part + 1) * cols],
                preferred_element_type=jnp.float32,
            ).astype(jnp.bfloat16)


def spread(puts, weights, group, own, other):
    arrays = (*own, other)
    slots, width = other.shape
    rows = puts.shape[1] // JOINED
    out = jax.ShapeDtypeStruct((rows, width // 2), jnp.bfloat16)
    spec = pl.BlockSpec(out.shape, lambda i: (0, 0))
    count = 2 * JOINED
    flat = pl.pallas_call(
        spread_kernel,
        grid=(1,),
        in_specs=[
            pl.BlockSpec((1, *puts.shape[1:]), lambda i: (group, 0, 0)),
            pl.BlockSpec((2, 1, slots, 1), lambda i: (0, group, 0, 0)),
        ]
        + [whole(a) for a in arrays],
        out_specs=[spec] * count,
        out_shape=[out] * count,
        cost_estimate=pl.CostEstimate(
            flops=4 * puts.shape[1] * slots * width, bytes_accessed=4 * puts.shape[1] * width, transcendentals=0
        ),
        compiler_params=params(),
        name="spread",
    )(puts, weights, *arrays)
    return [(flat[2 * i], flat[2 * i + 1]) for i in range(JOINED)]


def slot_tables(info, top_count, expert, capacity):
    sources, _, rows = info.shape
    wanted = jnp.stack([expert, expert ^ 1]).astype(jnp.float32)[:, None, None, None]
    match = info[None, :, :top_count] == wanted
    hit = jnp.any(match, 2)
    weights = info[:, top_count : 2 * top_count] + info[:, 2 * top_count : 3 * top_count] + info[:, 3 * top_count :]
    weight = jnp.sum(jnp.where(match, weights[None], 0.0), 2)
    order = jnp.arange(rows)
    before = jnp.dot(
        hit.astype(jnp.bfloat16).reshape(2 * sources, rows),
        (order[:, None] < order[None, :]).astype(jnp.bfloat16),
        preferred_element_type=jnp.float32,
    ).reshape(2, sources, rows)
    offset = ((jnp.arange(sources) % JOINED) * capacity)[None, :, None]
    place = jnp.where(hit, before.astype(jnp.int32) + offset, -1)
    groups = sources // JOINED
    place = place.reshape(2, groups, JOINED * rows)
    weight = weight.reshape(2, groups, 1, JOINED * rows)
    slots = jnp.arange(JOINED * capacity)
    picks = place[:, :, None, :] == slots[None, None, :, None]
    slot_weight = jnp.sum(jnp.where(picks, weight, 0.0), -1, keepdims=True)
    puts = place[:, :, :, None] == slots
    puts = jnp.concatenate([puts[0], puts[1]], axis=-1)
    return picks.astype(jnp.bfloat16), puts.astype(jnp.bfloat16), slot_weight


def query_units(queries, head_size, chips):
    rows, _, channels = queries.shape
    heads = channels // head_size
    own = jnp.transpose(queries, (1, 2, 0))
    both = jnp.concatenate([own, across(own, chips)], axis=2)
    keep = (jnp.arange(channels)[None, :] // head_size == jnp.arange(heads)[:, None])[None, :, :, None]
    return jnp.where(keep, both[:, None], jnp.zeros((), jnp.bfloat16)).reshape(2 * heads, channels, 2 * rows)


def pack(keys, values):
    rows = keys.shape[0]
    return jnp.concatenate([keys.reshape(rows, -1), values.T], axis=1)


def routing_rows(routes, route_weights, lanes):
    high = lax.reduce_precision(route_weights, exponent_bits=8, mantissa_bits=7)
    rest = route_weights - high
    middle = lax.reduce_precision(rest, exponent_bits=8, mantissa_bits=7)
    info = jnp.concatenate([routes.astype(jnp.float32), high, middle, rest - middle], axis=1).T.astype(jnp.bfloat16)
    return jnp.pad(info, ((0, -info.shape[0] % 16), (0, lanes - info.shape[1])))


def added(one, two):
    return (one.astype(jnp.float32) + two.astype(jnp.float32)).astype(jnp.bfloat16)


def gather_columns(own, got, parts):
    f_own, f_got = sideways(own, parts, 1), sideways(got, parts, 1)
    g_own, g_got = sideways(own, parts, -1), sideways(got, parts, -1)
    far_own, far_got = sideways(f_own, parts, 1), sideways(g_got, parts, -1)
    return [own, got, f_own, f_got, g_own, g_got, far_own, far_got]


def return_columns(done, parts, later):
    own, got, f_own, f_got, g_own, g_got, far_own, far_got = done
    u, v = sideways(far_own, parts, -1), sideways(far_got, parts, 1)
    w_got, x_own = sideways(f_got, parts, -1), sideways(g_own, parts, 1)
    sum_own, sum_got = added(f_own, u), added(g_got, v)
    if later is not None:
        (sum_own, sum_got), later = lax.optimization_barrier(((sum_own, sum_got), later))
    w_own, x_got = sideways(sum_own, parts, -1), sideways(sum_got, parts, 1)
    total = got.astype(jnp.float32) + w_got.astype(jnp.float32) + x_got.astype(jnp.float32)
    return (own, w_own, x_own), total.astype(jnp.bfloat16), later


def per_device(
    queries_a,
    keys_a,
    values_a,
    queries_b,
    keys_b,
    values_b,
    lambdas,
    head_gain_a,
    head_gain_b,
    out_a,
    out_b,
    residual,
    gain_mix,
    gain_pre,
    gain_post,
    routes,
    route_weights,
    expert_gate,
    expert_up,
    expert_down,
):
    heads_a = queries_a.shape[2] // DA
    heads_b = queries_b.shape[2] // DB
    head_slot = lax.axis_index("tp")
    seq_slot = lax.axis_index("sp")
    experts = lax.axis_size("sp")
    parts = lax.axis_size("tp")
    chips = experts // CORES
    half = chips // 2
    chip, core = seq_slot // CORES, seq_slot % CORES
    lambda_a = lax.dynamic_slice_in_dim(lambdas, head_slot * heads_a, heads_a)
    lambda_b = lax.dynamic_slice_in_dim(lambdas, HA + head_slot * heads_b, heads_b)
    sub_rows, width = residual.shape
    top_count = routes.shape[1]
    capacity = min(sub_rows, (5 * sub_rows * top_count + 4 * experts - 1) // (4 * experts))

    blocks = [pack(keys_a, values_a), pack(keys_b, values_b)]
    key_rows, lanes = blocks[0].shape
    blocks[0] = jnp.concatenate([blocks[0], routing_rows(routes, route_weights, lanes)], axis=0)
    routed_blocks = [blocks[0]]
    units = [query_units(queries_a, DA, chips), query_units(queries_b, DB, chips)]
    sizes = (DA, DB)
    first_flag = jnp.where(core == 0, 1, 0).astype(jnp.int32).reshape(1)
    states = [attend(units[i], sizes[i], first_flag, None, blocks[i : i + 1]) for i in range(2)]
    ahead, behind = list(blocks), list(blocks)
    for step in range(1, half + 1):
        seen_ahead = (chip >= step).astype(jnp.int32)
        seen_behind = (chip + step >= chips).astype(jnp.int32)
        for i in range(2):
            use, flags = [], []
            if step < half or i == 0:
                ahead[i] = along(ahead[i], chips, 1)
                use.append(ahead[i])
                flags.append(seen_ahead)
            if step < half or i == 1:
                behind[i] = along(behind[i], chips, -1)
                use.append(behind[i])
                flags.append(seen_behind)
            states[i] = attend(units[i], sizes[i], jnp.stack(flags), states[i], use)
            if i == 0:
                routed_blocks += use

    source_steps = [0] + [s for d in range(1, half) for s in (d, -d)] + [half]
    info = jnp.stack([b[key_rows : key_rows + 4 * top_count, :sub_rows] for b in routed_blocks]).astype(jnp.float32)
    tables = slot_tables(info, top_count, seq_slot, capacity)

    got = [across(states[i][1], chips) for i in range(2)]
    partial = merge(
        ((heads_a, 2 * DA), (heads_b, 2 * DB)),
        lambda_a, lambda_b, states[0][0], got[0], states[1][0], got[1], head_gain_a, head_gain_b, out_a, out_b,
    )
    mixed_rows = summed_on_arrival(partial, "tp", 0)
    after_mix = (residual.astype(jnp.float32) + rms_norm(mixed_rows, gain_mix)).astype(jnp.bfloat16)
    normed = rms_norm(after_mix.astype(jnp.float32), gain_pre).astype(jnp.bfloat16)
    normed, (picks, puts, slot_weight) = lax.optimization_barrier((normed, tables))

    ahead, behind = normed, normed
    sources = [(normed,)]
    columns = []

    def hold(*values):
        nonlocal ahead
        ahead, values = lax.optimization_barrier((ahead, values))
        return values

    def pick_group():
        k = len(columns)
        rows = pick(picks, k, sources[k * JOINED : (k + 1) * JOINED])
        (rows,) = hold(rows)
        columns.append(gather_columns(rows[0], across(rows[1], chips), parts))

    picked_at = []
    for step in range(1, half + 1):
        if step == half:
            ahead, behind = ahead[:, : width // 2], behind[:, width // 2 :]
        ahead, behind = along(ahead, chips, 1), along(behind, chips, -1)
        if step == 1:
            ahead, behind = lax.optimization_barrier((ahead, behind))
        if len(sources) >= (len(columns) + 1) * JOINED:
            pick_group()
            picked_at.append(step)
        for k, since in enumerate(picked_at):
            if step == since + 2:
                (columns[k][:6],) = hold(columns[k][:6])
            if step == since + 3:
                (columns[k][6:],) = hold(columns[k][6:])
        sources += [(ahead,), (behind,)] if step < half else [(ahead, behind)]
    pick_group()
    groups = len(columns)
    last = columns[-1]
    done = []
    after = last[0]
    if groups > 1:
        done = ffn(columns[:-1], expert_gate, expert_up, expert_down, after)
        after = done[-1][0]
    done = done + ffn([last], expert_gate, expert_up, expert_down, after)

    shares = {}
    for k in reversed(range(groups)):
        own_parts, other_sum, later = return_columns(done[k], parts, done[k - 1] if k else None)
        if k:
            done[k - 1] = later
        pairs = spread(puts, slot_weight, k, own_parts, across(other_sum, chips))
        for s, pair in zip(source_steps[k * JOINED : (k + 1) * JOINED], pairs):
            shares[s] = pair
    final = []
    for i in range(2):
        total = shares[0][i].astype(jnp.float32)
        for sign, reach in ((1, half - i), (-1, half - 1 + i)):
            carried = None
            for distance in range(reach, 0, -1):
                part = shares[half if distance == half else sign * distance][i]
                carried = along(part if carried is None else added(carried, part), chips, -sign)
            total = total + carried.astype(jnp.float32)
        final.append(total)
    routed = jnp.concatenate(final, axis=1)
    return (after_mix.astype(jnp.float32) + rms_norm(routed, gain_post)).astype(jnp.bfloat16)


def solution(mesh):
    in_specs = (
        P(("grp", "sp"), None, "tp"),
        P(("grp", "sp"), None, "tp"),
        P(("grp", "sp"), "tp"),
        P(("grp", "sp"), None, "tp"),
        P(("grp", "sp"), None, "tp"),
        P(("grp", "sp"), "tp"),
        P(),
        P(),
        P(),
        P("tp", None),
        P("tp", None),
        P(("grp", "sp", "tp"), None),
        P(),
        P(),
        P(),
        P(("grp", "sp", "tp"), None),
        P(("grp", "sp", "tp"), None),
        P("sp", None, "tp"),
        P("sp", None, "tp"),
        P("sp", "tp", None),
    )
    out_specs = P(("grp", "sp", "tp"), None)
    return jax.shard_map(
        per_device, mesh=mesh, in_specs=in_specs, out_specs=out_specs, check_vma=False
    )
```

```python
import functools

import jax
import jax.numpy as jnp
from jax import lax
from jax.experimental import pallas as pl
from jax.experimental.pallas import tpu as pltpu
from jax.sharding import PartitionSpec as P

HA = 4
DA = 128
DB = 64
CORES = 2
JOINED = 8
LOG2E = 1.4426950408889634
ROOM = 40 * 1024 * 1024


def along(array, chips, step):
    pairs = [(z * CORES + c, (z + step) % chips * CORES + c) for z in range(chips) for c in range(CORES)]
    return lax.ppermute(array, "sp", pairs)


def across(array, chips):
    return lax.ppermute(array, "sp", [(i, i ^ 1) for i in range(chips * CORES)])


def sideways(array, parts, step):
    return lax.ppermute(array, "tp", [(i, (i + step) % parts) for i in range(parts)])


def in_blocks(array, dim, devices):
    before, after = (array.shape[:dim], array.shape[dim + 1 :])
    return jnp.moveaxis(array.reshape(*before, devices, -1, *after), dim, 0)


def summed_on_arrival(array, axis, dim):
    devices = lax.axis_size(axis)
    blocks = lax.all_to_all(in_blocks(array, dim, devices), axis, 0, 0, tiled=True)
    return jnp.sum(blocks.astype(jnp.float32), axis=0)


def rms_norm(values, gain_vec):
    return values * lax.rsqrt(jnp.mean(values * values, -1, keepdims=True) + 1e-06) * gain_vec


def whole(array):
    return pl.BlockSpec(array.shape, lambda *_: (0,) * array.ndim)


def params():
    return pltpu.CompilerParams(vmem_limit_bytes=ROOM)


def absorb(n_units, width, scale, q_ref, kv_ref, block, states, causal):
    heads = n_units // 2
    channels = q_ref.shape[1]
    rows = states[0][1].shape[1]
    for u in range(n_units):
        map_at, head = u // heads, u % heads
        keys = kv_ref[block, :rows, map_at * channels : (map_at + 1) * channels]
        vals = kv_ref[block, head * width : (head + 1) * width, 2 * channels :]
        base = u * (width + 16)
        for at, state in states:
            scores = (
                jnp.dot(keys, q_ref[u, :, at * rows : (at + 1) * rows], preferred_element_type=jnp.float32) * scale
            )
            if causal:
                key_pos = lax.broadcasted_iota(jnp.int32, scores.shape, 0)
                query_pos = lax.broadcasted_iota(jnp.int32, scores.shape, 1)
                scores = jnp.where(key_pos <= query_pos, scores, -1e30)
            top_rows, total_rows = slice(base + width, base + width + 8), slice(base + width + 8, base + width + 16)
            old = state[top_rows]
            new = jnp.maximum(old, jnp.max(scores, axis=0, keepdims=True))
            terms = jnp.exp2(scores - new[:1])
            shrink = jnp.exp2(old - new)
            state[top_rows] = new
            state[total_rows] = state[total_rows] * shrink + jnp.sum(terms, axis=0, keepdims=True)
            place = slice(base, base + width)
            state[place] = state[place] * shrink[:1] + jnp.dot(
                vals, terms.astype(jnp.bfloat16), preferred_element_type=jnp.float32
            )


def first_kernel(n_units, width, scale, flags, q_ref, kv_ref, own_ref, other_ref):
    for u in range(n_units):
        base = u * (width + 16)
        for state in (own_ref, other_ref):
            state[base : base + width + 16] = jnp.zeros((width + 16, state.shape[1]), jnp.float32)
            state[base + width : base + width + 8] = jnp.full((8, state.shape[1]), -1e30, jnp.float32)
    absorb(n_units, width, scale, q_ref, kv_ref, 0, ((0, own_ref),), True)

    @pl.when(flags[0] > 0)
    def _():
        absorb(n_units, width, scale, q_ref, kv_ref, 0, ((1, other_ref),), False)


def step_kernel(n_units, width, scale, n_blocks, flags, q_ref, own_in, other_in, *refs):
    blocks, (own_ref, other_ref, kv_ref) = refs[:n_blocks], refs[n_blocks:]
    own_ref[...] = own_in[...]
    other_ref[...] = other_in[...]
    for i in range(n_blocks):
        kv_ref[i] = blocks[i][...]

    @pl.loop(0, n_blocks)
    def _(i):
        @pl.when(flags[i] > 0)
        def _():
            absorb(n_units, width, scale, q_ref, kv_ref, i, ((0, own_ref), (1, other_ref)), False)


def attend(units, head_size, flags, state, blocks):
    n_units, channels, both = units.shape
    width = 2 * head_size
    rows = both // 2
    scale = head_size ** (-0.5) * LOG2E
    shape = jax.ShapeDtypeStruct((n_units * (width + 16), rows), jnp.float32)
    if state is None:
        kernel = functools.partial(first_kernel, n_units, width, scale)
        operands = (units, blocks[0][None])
        scratch = []
    else:
        kernel = functools.partial(step_kernel, n_units, width, scale, len(blocks))
        operands = (units, *state, *blocks)
        scratch = [pltpu.VMEM((len(blocks), *blocks[0].shape), jnp.bfloat16)]
    spec = pl.BlockSpec(shape.shape, lambda *_: (0, 0))
    work = len(blocks) * rows * both * n_units
    return pl.pallas_call(
        kernel,
        grid_spec=pltpu.PrefetchScalarGridSpec(
            num_scalar_prefetch=1,
            grid=(1,),
            in_specs=[whole(a) for a in operands],
            out_specs=[spec, spec],
            scratch_shapes=scratch,
        ),
        out_shape=[shape, shape],
        input_output_aliases={} if state is None else {2: 0, 3: 1},
        cost_estimate=pl.CostEstimate(
            flops=4 * work * (channels + width), bytes_accessed=6 * shape.size * 4, transcendentals=work
        ),
        compiler_params=params(),
        name="attend",
    )(flags, *operands)


def merge_kernel(sizes, lam_a, lam_b, own_a, got_a, own_b, got_b, gain_a, gain_b, proj_a, proj_b, out_ref):
    result = None
    groups = ((lam_a, own_a, got_a, gain_a, proj_a), (lam_b, own_b, got_b, gain_b, proj_b))
    for (heads, width), (lam, own, got, gain, proj) in zip(sizes, groups):

        def share(u):
            base = u * (width + 16)
            at = base + width
            one, two = own[at : at + 1], got[at : at + 1]
            top = jnp.maximum(one, two)
            one, two = jnp.exp2(one - top), jnp.exp2(two - top)
            at = at + 8
            total = own[at : at + 1] * one + got[at : at + 1] * two
            place = slice(base, base + width)
            return (own[place] * one + got[place] * two) / total

        for head in range(heads):
            mix = share(head) - lam[head] * share(heads + head)
            mean = jnp.mean(mix * mix, axis=0, keepdims=True)
            normed = (mix * lax.rsqrt(mean + 1e-6) * gain[...]).T.astype(jnp.bfloat16)
            part = jnp.dot(normed, proj[head * width : (head + 1) * width], preferred_element_type=jnp.float32)
            result = part if result is None else result + part
    out_ref[...] = result.astype(jnp.bfloat16)


def merge(sizes, lam_a, lam_b, own_a, got_a, own_b, got_b, gain_a, gain_b, proj_a, proj_b):
    rows = own_a.shape[1]
    operands = (own_a, got_a, own_b, got_b, gain_a.reshape(-1, 1), gain_b.reshape(-1, 1), proj_a, proj_b)
    out = jax.ShapeDtypeStruct((rows, proj_a.shape[1]), jnp.bfloat16)
    return pl.pallas_call(
        functools.partial(merge_kernel, sizes),
        grid=(1,),
        in_specs=[pl.BlockSpec(memory_space=pltpu.SMEM)] * 2 + [whole(a) for a in operands],
        out_specs=pl.BlockSpec(out.shape, lambda i: (0, 0)),
        out_shape=out,
        cost_estimate=pl.CostEstimate(
            flops=4 * rows * proj_a.size, bytes_accessed=8 * proj_a.size, transcendentals=0
        ),
        compiler_params=params(),
        name="merge",
    )(lam_a, lam_b, *operands)


def stacked(refs):
    return jnp.concatenate([r[...].astype(jnp.float32) for r in refs], axis=0).astype(jnp.bfloat16)


def ffn_kernel(count, tile, gate_ref, up_ref, down_ref, *refs):
    ins, outs, (rows_ref, sum_ref) = refs[:count], refs[count : 2 * count], refs[-2:]
    half = pl.program_id(0)
    each = ins[0].shape[0]
    together = tile // each

    @pl.when(half == 0)
    def _():
        for i in range(0, count, together):
            rows_ref[i * each : i * each + tile] = stacked(ins[i : i + together])

    @pl.loop(0, count // together)
    def _(i):
        place = pl.ds(pl.multiple_of(i * tile, tile), tile)
        x = rows_ref[place]
        gate_pre = jnp.dot(x, gate_ref[0], preferred_element_type=jnp.float32)
        up_pre = jnp.dot(x, up_ref[0], preferred_element_type=jnp.float32)
        glu_part = jnp.minimum(gate_pre, 7.0)
        lin_part = jnp.clip(up_pre, -7.0, 7.0)
        hidden = (glu_part * jax.nn.sigmoid(1.702 * glu_part) * (lin_part + 1.0)).astype(jnp.bfloat16)
        part = jnp.dot(hidden, down_ref[0], preferred_element_type=jnp.float32)

        @pl.when(half == 0)
        def _():
            sum_ref[place] = part

        @pl.when(half == 1)
        def _():
            sum_ref[place] = sum_ref[place] + part

    @pl.when(half == 1)
    def _():
        for i in range(count):
            outs[i][...] = sum_ref[i * each : (i + 1) * each].astype(jnp.bfloat16)


def ffn(groups, gate, up, down, after):
    arrays = [a for group in groups for a in group]
    count = len(arrays)
    each, width = arrays[0].shape
    hidden = gate.shape[2]
    per = hidden // 2
    rows = each * count

    def kernel(*refs):
        ffn_kernel(count, each * 4, *refs[:3], *refs[4:])

    out = pl.pallas_call(
        kernel,
        grid=(2,),
        in_specs=[
            pl.BlockSpec((1, width, per), lambda i: (0, 0, i)),
            pl.BlockSpec((1, width, per), lambda i: (0, 0, i)),
            pl.BlockSpec((1, per, width), lambda i: (0, i, 0)),
            pl.BlockSpec(memory_space=pl.ANY),
        ]
        + [whole(a) for a in arrays],
        out_specs=[whole(a) for a in arrays],
        out_shape=[jax.ShapeDtypeStruct(a.shape, jnp.bfloat16) for a in arrays],
        scratch_shapes=[pltpu.VMEM((rows, width), jnp.bfloat16), pltpu.VMEM((rows, width), jnp.float32)],
        cost_estimate=pl.CostEstimate(
            flops=6 * rows * width * hidden, bytes_accessed=4 * rows * width + 6 * width * hidden, transcendentals=rows * hidden
        ),
        compiler_params=pltpu.CompilerParams(vmem_limit_bytes=56 * 1024 * 1024),
        name="expert",
    )(gate, up, down, after, *arrays)
    return [out[i : i + 8] for i in range(0, count, 8)]


def pick_kernel(counts, picks_ref, *refs):
    outs, at, rows = refs[-2:], 0, []
    for count in counts:
        pieces = [r[...] for r in refs[at : at + count]]
        rows.append(pieces[0] if count == 1 else jnp.concatenate(pieces, axis=1))
        at += count
    rows = jnp.concatenate(rows, axis=0)
    for p in range(2):
        outs[p][...] = jnp.dot(picks_ref[p, 0], rows, preferred_element_type=jnp.float32).astype(jnp.bfloat16)


def pick(picks, group, sources):
    arrays = [a for pieces in sources for a in pieces]
    slots = picks.shape[2]
    width = sum(a.shape[1] for a in sources[0])
    out = jax.ShapeDtypeStruct((slots, width), jnp.bfloat16)
    spec = pl.BlockSpec(out.shape, lambda i: (0, 0))
    return pl.pallas_call(
        functools.partial(pick_kernel, [len(pieces) for pieces in sources]),
        grid=(1,),
        in_specs=[pl.BlockSpec((2, 1, *picks.shape[2:]), lambda i: (0, group, 0, 0))] + [whole(a) for a in arrays],
        out_specs=[spec, spec],
        out_shape=[out, out],
        cost_estimate=pl.CostEstimate(
            flops=4 * slots * picks.shape[3] * width, bytes_accessed=4 * picks.shape[3] * width, transcendentals=0
        ),
        compiler_params=params(),
        name="pick",
    )(picks, *arrays)


def spread_kernel(puts_ref, weight_ref, *refs):
    ins, outs = refs[:4], refs[4:]
    own = sum(r[...].astype(jnp.float32) for r in ins[:3]) * weight_ref[0, 0]
    other = ins[3][...].astype(jnp.float32) * weight_ref[1, 0]
    slots = jnp.concatenate([own, other], axis=0).astype(jnp.bfloat16)
    rows, cols = outs[0].shape
    for i in range(len(outs) // 2):
        for part in range(2):
            outs[2 * i + part][...] = jnp.dot(
                puts_ref[0, i * rows : (i + 1) * rows],
                slots[:, part * cols : (part + 1) * cols],
                preferred_element_type=jnp.float32,
            ).astype(jnp.bfloat16)


def spread(puts, weights, group, own, other):
    arrays = (*own, other)
    slots, width = other.shape
    rows = puts.shape[1] // JOINED
    out = jax.ShapeDtypeStruct((rows, width // 2), jnp.bfloat16)
    spec = pl.BlockSpec(out.shape, lambda i: (0, 0))
    count = 2 * JOINED
    flat = pl.pallas_call(
        spread_kernel,
        grid=(1,),
        in_specs=[
            pl.BlockSpec((1, *puts.shape[1:]), lambda i: (group, 0, 0)),
            pl.BlockSpec((2, 1, slots, 1), lambda i: (0, group, 0, 0)),
        ]
        + [whole(a) for a in arrays],
        out_specs=[spec] * count,
        out_shape=[out] * count,
        cost_estimate=pl.CostEstimate(
            flops=4 * puts.shape[1] * slots * width, bytes_accessed=4 * puts.shape[1] * width, transcendentals=0
        ),
        compiler_params=params(),
        name="spread",
    )(puts, weights, *arrays)
    return [(flat[2 * i], flat[2 * i + 1]) for i in range(JOINED)]


def slot_tables(info, top_count, expert, capacity):
    sources, _, rows = info.shape
    wanted = jnp.stack([expert, expert ^ 1]).astype(jnp.float32)[:, None, None, None]
    match = info[None, :, :top_count] == wanted
    hit = jnp.any(match, 2)
    weights = info[:, top_count : 2 * top_count] + info[:, 2 * top_count : 3 * top_count] + info[:, 3 * top_count :]
    weight = jnp.sum(jnp.where(match, weights[None], 0.0), 2)
    order = jnp.arange(rows)
    before = jnp.dot(
        hit.astype(jnp.bfloat16).reshape(2 * sources, rows),
        (order[:, None] < order[None, :]).astype(jnp.bfloat16),
        preferred_element_type=jnp.float32,
    ).reshape(2, sources, rows)
    offset = ((jnp.arange(sources) % JOINED) * capacity)[None, :, None]
    place = jnp.where(hit, before.astype(jnp.int32) + offset, -1)
    groups = sources // JOINED
    place = place.reshape(2, groups, JOINED * rows)
    weight = weight.reshape(2, groups, 1, JOINED * rows)
    slots = jnp.arange(JOINED * capacity)
    picks = place[:, :, None, :] == slots[None, None, :, None]
    slot_weight = jnp.sum(jnp.where(picks, weight, 0.0), -1, keepdims=True)
    puts = place[:, :, :, None] == slots
    puts = jnp.concatenate([puts[0], puts[1]], axis=-1)
    return picks.astype(jnp.bfloat16), puts.astype(jnp.bfloat16), slot_weight


def query_units(queries, head_size, chips):
    rows, _, channels = queries.shape
    heads = channels // head_size
    own = jnp.transpose(queries, (1, 2, 0))
    both = jnp.concatenate([own, across(own, chips)], axis=2)
    keep = (jnp.arange(channels)[None, :] // head_size == jnp.arange(heads)[:, None])[None, :, :, None]
    return jnp.where(keep, both[:, None], jnp.zeros((), jnp.bfloat16)).reshape(2 * heads, channels, 2 * rows)


def pack(keys, values):
    rows = keys.shape[0]
    return jnp.concatenate([keys.reshape(rows, -1), values.T], axis=1)


def routing_rows(routes, route_weights, lanes):
    high = lax.reduce_precision(route_weights, exponent_bits=8, mantissa_bits=7)
    rest = route_weights - high
    middle = lax.reduce_precision(rest, exponent_bits=8, mantissa_bits=7)
    info = jnp.concatenate([routes.astype(jnp.float32), high, middle, rest - middle], axis=1).T.astype(jnp.bfloat16)
    return jnp.pad(info, ((0, -info.shape[0] % 16), (0, lanes - info.shape[1])))


def added(one, two):
    return (one.astype(jnp.float32) + two.astype(jnp.float32)).astype(jnp.bfloat16)


def gather_columns(own, got, parts):
    f_own, f_got = sideways(own, parts, 1), sideways(got, parts, 1)
    g_own, g_got = sideways(own, parts, -1), sideways(got, parts, -1)
    far_own, far_got = sideways(f_own, parts, 1), sideways(g_got, parts, -1)
    return [own, got, f_own, f_got, g_own, g_got, far_own, far_got]


def return_columns(done, parts, later, held):
    own, got, f_own, f_got, g_own, g_got, far_own, far_got = done
    u, v = sideways(far_own, parts, -1), sideways(far_got, parts, 1)
    w_got, x_own = sideways(f_got, parts, -1), sideways(g_own, parts, 1)
    (u, v), held = lax.optimization_barrier(((u, v), held))
    w_own, x_got = sideways(added(f_own, u), parts, -1), sideways(added(g_got, v), parts, 1)
    total = got.astype(jnp.float32) + w_got.astype(jnp.float32) + x_got.astype(jnp.float32)
    total = total.astype(jnp.bfloat16)
    if later is not None:
        (w_own, x_own, total), later = lax.optimization_barrier(((w_own, x_own, total), later))
    return (own, w_own, x_own), total, later, held


def per_device(
    queries_a,
    keys_a,
    values_a,
    queries_b,
    keys_b,
    values_b,
    lambdas,
    head_gain_a,
    head_gain_b,
    out_a,
    out_b,
    residual,
    gain_mix,
    gain_pre,
    gain_post,
    routes,
    route_weights,
    expert_gate,
    expert_up,
    expert_down,
):
    heads_a = queries_a.shape[2] // DA
    heads_b = queries_b.shape[2] // DB
    head_slot = lax.axis_index("tp")
    seq_slot = lax.axis_index("sp")
    experts = lax.axis_size("sp")
    parts = lax.axis_size("tp")
    chips = experts // CORES
    half = chips // 2
    chip, core = seq_slot // CORES, seq_slot % CORES
    lambda_a = lax.dynamic_slice_in_dim(lambdas, head_slot * heads_a, heads_a)
    lambda_b = lax.dynamic_slice_in_dim(lambdas, HA + head_slot * heads_b, heads_b)
    sub_rows, width = residual.shape
    top_count = routes.shape[1]
    capacity = min(sub_rows, (5 * sub_rows * top_count + 4 * experts - 1) // (4 * experts))

    blocks = [pack(keys_a, values_a), pack(keys_b, values_b)]
    key_rows, lanes = blocks[0].shape
    blocks[0] = jnp.concatenate([blocks[0], routing_rows(routes, route_weights, lanes)], axis=0)
    routed_blocks = [blocks[0]]
    units = [query_units(queries_a, DA, chips), query_units(queries_b, DB, chips)]
    sizes = (DA, DB)
    first_flag = jnp.where(core == 0, 1, 0).astype(jnp.int32).reshape(1)
    states = [attend(units[i], sizes[i], first_flag, None, blocks[i : i + 1]) for i in range(2)]
    ahead, behind = list(blocks), list(blocks)
    for step in range(1, half + 1):
        seen_ahead = (chip >= step).astype(jnp.int32)
        seen_behind = (chip + step >= chips).astype(jnp.int32)
        for i in range(2):
            use, flags = [], []
            if step < half or i == 0:
                ahead[i] = along(ahead[i], chips, 1)
                use.append(ahead[i])
                flags.append(seen_ahead)
            if step < half or i == 1:
                behind[i] = along(behind[i], chips, -1)
                use.append(behind[i])
                flags.append(seen_behind)
            states[i] = attend(units[i], sizes[i], jnp.stack(flags), states[i], use)
            if i == 0:
                routed_blocks += use

    source_steps = [0] + [s for d in range(1, half) for s in (d, -d)] + [half]
    info = jnp.stack([b[key_rows : key_rows + 4 * top_count, :sub_rows] for b in routed_blocks]).astype(jnp.float32)
    tables = slot_tables(info, top_count, seq_slot, capacity)

    got = [across(states[i][1], chips) for i in range(2)]
    partial = merge(
        ((heads_a, 2 * DA), (heads_b, 2 * DB)),
        lambda_a, lambda_b, states[0][0], got[0], states[1][0], got[1], head_gain_a, head_gain_b, out_a, out_b,
    )
    mixed_rows = summed_on_arrival(partial, "tp", 0)
    after_mix = (residual.astype(jnp.float32) + rms_norm(mixed_rows, gain_mix)).astype(jnp.bfloat16)
    normed = rms_norm(after_mix.astype(jnp.float32), gain_pre).astype(jnp.bfloat16)
    normed, (picks, puts, slot_weight) = lax.optimization_barrier((normed, tables))

    ahead, behind = normed, normed
    sources = [(normed,)]
    columns = []

    def hold(*values):
        nonlocal ahead
        ahead, values = lax.optimization_barrier((ahead, values))
        return values

    def pick_group():
        k = len(columns)
        rows = pick(picks, k, sources[k * JOINED : (k + 1) * JOINED])
        (rows,) = hold(rows)
        columns.append(gather_columns(rows[0], across(rows[1], chips), parts))

    picked_at = []
    for step in range(1, half + 1):
        if step == half:
            ahead, behind = ahead[:, : width // 2], behind[:, width // 2 :]
        ahead, behind = along(ahead, chips, 1), along(behind, chips, -1)
        if step == 1:
            ahead, behind = lax.optimization_barrier((ahead, behind))
        if len(sources) >= (len(columns) + 1) * JOINED:
            pick_group()
            picked_at.append(step)
        for k, since in enumerate(picked_at):
            if step == since + 2:
                (columns[k][:6],) = hold(columns[k][:6])
            if step == since + 3:
                (columns[k][6:],) = hold(columns[k][6:])
        sources += [(ahead,), (behind,)] if step < half else [(ahead, behind)]
    pick_group()
    groups = len(columns)
    last = columns[-1]
    done = []
    after = last[0]
    if groups > 1:
        done = ffn(columns[:-1], expert_gate, expert_up, expert_down, after)
        after = done[-1][0]
    done = done + ffn([last], expert_gate, expert_up, expert_down, after)

    shares, carried = {}, {}
    reach = {(i, sign): half - i if sign == 1 else half - 1 + i for i in range(2) for sign in (1, -1)}

    def send(key, distance):
        i, sign = key
        part = shares[half if distance == half else sign * distance][i]
        carried[key] = along(added(carried[key], part) if key in carried else part, chips, -sign)

    for k in reversed(range(groups)):
        own_parts, other_sum, later, held = return_columns(done[k], parts, done[k - 1] if k else None, carried)
        carried = dict(held)
        if k:
            done[k - 1] = later
        pairs = spread(puts, slot_weight, k, own_parts, across(other_sum, chips))
        for s, pair in zip(source_steps[k * JOINED : (k + 1) * JOINED], pairs):
            shares[s] = pair
        if k == groups - 1:
            for key, distance in reach.items():
                send(key, distance)
    for key, distance in reach.items():
        for nearer in range(distance - 1, 0, -1):
            send(key, nearer)
    final = [
        shares[0][i].astype(jnp.float32) + carried[i, 1].astype(jnp.float32) + carried[i, -1].astype(jnp.float32)
        for i in range(2)
    ]
    routed = jnp.concatenate(final, axis=1)
    return (after_mix.astype(jnp.float32) + rms_norm(routed, gain_post)).astype(jnp.bfloat16)


def solution(mesh):
    in_specs = (
        P(("grp", "sp"), None, "tp"),
        P(("grp", "sp"), None, "tp"),
        P(("grp", "sp"), "tp"),
        P(("grp", "sp"), None, "tp"),
        P(("grp", "sp"), None, "tp"),
        P(("grp", "sp"), "tp"),
        P(),
        P(),
        P(),
        P("tp", None),
        P("tp", None),
        P(("grp", "sp", "tp"), None),
        P(),
        P(),
        P(),
        P(("grp", "sp", "tp"), None),
        P(("grp", "sp", "tp"), None),
        P("sp", None, "tp"),
        P("sp", None, "tp"),
        P("sp", "tp", None),
    )
    out_specs = P(("grp", "sp", "tp"), None)
    return jax.shard_map(
        per_device, mesh=mesh, in_specs=in_specs, out_specs=out_specs, check_vma=False
    )
```
